512 devices in a mesh: ep: 128 (over z, x, core), tp: 4 (over y).
Axes of the slice: x: 4, y: 4, z: 16, core: 2. Of those that a mesh axis runs over, the one named last changes fastest.
Arguments:
- tokens: bfloat16 [512, 2048], P('ep', 'tp'), may hold values from -6 to 6
- norm_gain: bfloat16 [2048], P('tp'), may hold values from 0.099609375 to 1.8984375
- w_query: bfloat16 [2048, 2048], P('tp', 'ep'), may hold values from -0.125 to 0.125
- w_forget: bfloat16 [2048, 2048], P('tp', 'ep'), may hold values from -0.125 to 0.125
- w_input: bfloat16 [2048, 2048], P('tp', 'ep'), may hold values from -0.125 to 0.125
- forget_floor: float32 [2048], P('tp'), may hold values from 0 to 0.9
- head_gain: bfloat16 [128], replicated, may hold values from 0.099609375 to 1.8984375
- w_output: bfloat16 [2048, 2048], P('tp', 'ep'), may hold values from -0.125 to 0.125
- state: float32 [512, 16, 128, 128], P('ep', 'tp'), may hold values from -6 to 6
- ffn_gain: bfloat16 [2048], P('tp'), may hold values from 0.099609375 to 1.8984375
- route_experts: int32 [512, 2], P('ep'), may hold values from 0 to 7, all different within a row; in each aligned block of 4 rows (0 to 3, 4 to 7, ...) at most 2 rows name the same one
- route_weights: float32 [512, 2], P('ep'), may hold values from 0.1 to 1
- w_gate: bfloat16 [128, 2048, 448], P('ep', None, 'tp'), may hold values from -0.125 to 0.125
- w_up: bfloat16 [128, 2048, 448], P('ep', None, 'tp'), may hold values from -0.125 to 0.125
- w_down: bfloat16 [128, 448, 2048], P('ep', 'tp'), may hold values from -0.0625 to 0.0625
Outputs:
- mixed: bfloat16 [512, 2048], P('ep', 'tp')
- new_state: float32 [512, 16, 128, 128], P('ep', 'tp')
The draws below stay inside these ranges and needn't reach their ends.
Inputs may be any that keep to these rules, and one draw needn't show every extreme that they name: `route_experts`: each row names two different experts. Among the rows of one index of ep, no expert is named by more than 2 rows, and in every draw some expert is named by exactly 2 of them.
All inputs are finite; a program needn't handle non-finite values.
Results may differ from the reference program's by a relative error of at most 0.014.
Values may be sent and summed in bfloat16 or wider, within the bound.
No kernel may reach another device: no remote copies, remote signals or barrier semaphores. Data moves between devices by JAX's collectives and lax.ppermute only.
A program may use at most 64 MiB of HBM per device.

```python
import math
import jax
import jax.numpy as jnp
import numpy as np
from jax import lax

D = 2048
HEADS = 16
HEAD = 128
FF_E = 7168
EXPERTS = 8
SEQ_DEV = 4
EP_SPAN = 16
TOKENS = 512
CAP = 2
N_EP = 128


def shard_levels(own_key, dims, shards, least, top_value):
    factor_of = 1.0
    for axis_at, parts in shards:
        heights = jax.random.uniform(jax.random.fold_in(jax.random.fold_in(own_key, 6), axis_at), (parts,), jnp.float32, least / len(shards), top_value / len(shards))
        factor_of = factor_of * jnp.repeat(jnp.exp(heights), dims[axis_at] // parts).reshape((-1,) + (1,) * (len(dims) - 1 - axis_at))
    return factor_of


def assign_block(own_key, own, number, rows, number_of, top, limit, lean):
    order = jax.random.permutation(own_key, number_of)
    packed, common = load_shares(number_of, rows * top, limit, lean, True), load_shares(number_of, rows * top, limit, lean, False)
    places = jnp.arange(number_of)

    def named(sizes, turn):
        used = int((sizes > 0).sum())
        fixed = max(1, used // 4)
        moved = fixed + (places - fixed + turn * (used - fixed)) % max(1, number_of - fixed)
        return jnp.zeros((number_of,), jnp.int32).at[order[jnp.where(places < fixed, places, moved)]].set(jnp.asarray(sizes, jnp.int32))

    sizes = jnp.where(number % 4 == 0, named(packed, number // 4), named(common, number - number // 4 - 1))
    mixed = jax.random.permutation(jax.random.fold_in(own, 3), number_of)
    donor, sink = mixed[0:number_of // 2 * 2:2], mixed[1:number_of // 2 * 2:2]
    room = jnp.minimum(sizes[donor] - 1, limit - sizes[sink]) // 2
    room = jnp.where((donor == order[0]) | (sink == order[0]) | (sizes[sink] == 0), 0, jnp.maximum(room, 0))
    moved = jax.random.randint(jax.random.fold_in(own, 4), (number_of // 2,), 0, 1 << 20) % (room + 1)
    sizes = sizes.at[donor].add(-moved).at[sink].add(moved)
    items = jnp.searchsorted(jnp.cumsum(sizes), jnp.arange(rows * top), side="right").astype(jnp.int32)
    listing = items.reshape(top, rows).T
    listing = listing[jax.random.permutation(jax.random.fold_in(own, 1), rows)]
    turn = jax.random.randint(jax.random.fold_in(own, 2), (rows, 1), 0, top)
    return jnp.take_along_axis(listing, (jnp.arange(top)[None, :] + turn) % top, axis=1)


def load_shares(amount, total, most, lean, full):
    loads = [(1 << 20) // math.isqrt(rank ** lean) + 1 for rank in range(1, amount + 1)]
    largest = most if full else min(most, max(-(-total // amount), total * loads[0] // sum(loads)))
    least = 1 if total - largest >= amount - 1 else 0
    holding, spare = [largest] + [least] * (amount - 1), total - largest - least * (amount - 1)
    while spare > 0:
        movable = [i for i in range(1, amount) if holding[i] < largest] or [i for i in range(1, amount) if holding[i] < most]
        whole, left = sum([loads[i] for i in movable]), spare
        for i in movable:
            extra = min(most - holding[i], max(1, left * loads[i] // whole), spare)
            holding[i] = holding[i] + extra
            spare = spare - extra
    return np.array(holding)


def scatter_about(rng, dims, width, bound, shards=(), held_as=jnp.bfloat16):
    result = jax.random.normal(rng, dims, jnp.float32) * width
    if len(shards) > 0:
        result = shard_levels(rng, dims, shards, -0.22, 0.18) * result
    return jnp.clip(result, min=-bound, max=bound).astype(held_as)


def setup_inputs(seed: int = 0) -> dict:
    seeds = jax.random.split(jax.random.key(seed), 16)
    tokens = scatter_about(seeds[0], (TOKENS, D), 1.0, 6.0, ((0, 128), (1, 4)))
    norm_gain = jnp.clip(1.0 + 0.18 * jax.random.normal(seeds[1], (D,), jnp.float32), 0.099609375, 1.8984375).astype(jnp.bfloat16)
    w_query = scatter_about(seeds[2], (D, HEADS * HEAD), D ** -0.5, 0.125, ((0, 4), (1, 128)))
    w_forget = scatter_about(seeds[3], (D, HEADS * HEAD), D ** -0.5, 0.125, ((0, 4), (1, 128)))
    w_input = scatter_about(seeds[4], (D, HEADS * HEAD), D ** -0.5, 0.125, ((0, 4), (1, 128)))
    forget_floor = jnp.clip(0.9 * jax.random.uniform(seeds[5], (HEADS * HEAD,), jnp.float32) ** shard_levels(seeds[5], (HEADS * HEAD,), ((0, 4),), -0.2, 0.2), 0.0, 0.9)
    head_gain = jnp.clip(1.0 + 0.18 * jax.random.normal(seeds[6], (HEAD,), jnp.float32), 0.099609375, 1.8984375).astype(jnp.bfloat16)
    w_output = scatter_about(seeds[7], (HEADS * HEAD, D), (HEADS * HEAD) ** -0.5, 0.125, ((0, 4), (1, 128)))
    state = scatter_about(seeds[8], (TOKENS, HEADS, HEAD, HEAD), 1.0, 6.0, ((0, 128), (1, 4)), jnp.float32)
    ffn_gain = jnp.clip(1.0 + 0.18 * jax.random.normal(seeds[9], (D,), jnp.float32), 0.099609375, 1.8984375).astype(jnp.bfloat16)
    route_experts_keys = jax.random.split(jax.random.fold_in(seeds[10], 1), TOKENS // SEQ_DEV)
    route_experts_turns = jax.random.permutation(jax.random.fold_in(seeds[10], 3), TOKENS // SEQ_DEV)
    route_experts = jax.vmap(lambda own, number: assign_block(jax.random.fold_in(seeds[10], 2), own, number, SEQ_DEV, EXPERTS, 2, CAP, 0))(route_experts_keys, route_experts_turns).reshape((TOKENS, 2))
    route_weights = jnp.clip(0.1 + 0.9 * jax.random.uniform(seeds[11], (TOKENS, 2), jnp.float32) ** shard_levels(seeds[11], (TOKENS, 2), ((0, 128),), -0.2, 0.2), 0.1, 1.0)
    w_gate = scatter_about(seeds[12], (N_EP, D, FF_E // EP_SPAN), D ** -0.5, 0.125, ((0, 128), (2, 4)))
    w_up = scatter_about(seeds[13], (N_EP, D, FF_E // EP_SPAN), D ** -0.5, 0.125, ((0, 128), (2, 4)))
    w_down = scatter_about(seeds[14], (N_EP, FF_E // EP_SPAN, D), FF_E ** -0.5, 0.0625, ((0, 128), (1, 4)))
    return {"tokens": tokens, "norm_gain": norm_gain, "w_query": w_query, "w_forget": w_forget, "w_input": w_input, "forget_floor": forget_floor, "head_gain": head_gain, "w_output": w_output, "state": state, "ffn_gain": ffn_gain, "route_experts": route_experts, "route_weights": route_weights, "w_gate": w_gate, "w_up": w_up, "w_down": w_down}


EPS = 1e-06

def norm_rows(values, gain):
    mean_sq = lax.optimization_barrier(jnp.mean(values * values, axis=-1, keepdims=True))
    return values * lax.rsqrt(mean_sq + EPS) * gain.astype(jnp.float32)

def reference(tokens, norm_gain, w_query, w_forget, w_input, forget_floor, head_gain, w_output, state, ffn_gain, route_experts, route_weights, w_gate, w_up, w_down):
    tok_f32 = tokens.astype(jnp.float32)
    batch = tokens.shape[0]
    normed = norm_rows(tok_f32, norm_gain).astype(jnp.bfloat16)
    queries = jnp.dot(normed, w_query, preferred_element_type=jnp.float32).reshape(batch, HEADS, HEAD)
    fgate = jnp.dot(normed, w_forget, preferred_element_type=jnp.float32).reshape(batch, HEADS, HEAD)
    inputs = jnp.dot(normed, w_input, preferred_element_type=jnp.float32).reshape(batch, HEADS, HEAD)
    floors = forget_floor.reshape(HEADS, HEAD)
    forget = floors + (1.0 - floors) * jax.nn.sigmoid(fgate)
    new_state = forget[..., None] * state + (1.0 - forget)[..., None] * inputs[:, :, None, :]
    reads = jnp.einsum('bhk,bhkv->bhv', jax.nn.silu(queries), new_state, precision=lax.Precision.HIGHEST)
    heads_out = norm_rows(reads, head_gain).reshape(batch, HEADS * HEAD).astype(jnp.bfloat16)
    mixer_out = jnp.dot(heads_out, w_output, preferred_element_type=jnp.float32).astype(jnp.bfloat16)
    middle = (tok_f32 + mixer_out.astype(jnp.float32)).astype(jnp.bfloat16)
    second = norm_rows(middle.astype(jnp.float32), ffn_gain).astype(jnp.bfloat16)
    second = lax.optimization_barrier(second)
    top_count = route_experts.shape[1]
    flat_experts = route_experts.reshape(-1).astype(jnp.int32)
    flat_weights = route_weights.reshape(-1)

    def one_route(item_index):
        token_index = item_index // top_count
        expert = flat_experts[item_index]
        start = (expert * EP_SPAN).astype(jnp.int32)
        gate_piece = lax.dynamic_slice_in_dim(w_gate, start, EP_SPAN, 0).astype(jnp.float32)
        up_piece = lax.dynamic_slice_in_dim(w_up, start, EP_SPAN, 0).astype(jnp.float32)
        down_piece = lax.dynamic_slice_in_dim(w_down, start, EP_SPAN, 0).astype(jnp.float32)
        token_row = second[token_index].astype(jnp.float32)
        gate_act = jnp.einsum('d,jdf->jf', token_row, gate_piece)
        up_act = jnp.einsum('d,jdf->jf', token_row, up_piece)
        hidden = (jax.nn.silu(gate_act) * up_act).astype(jnp.bfloat16)
        hidden = lax.optimization_barrier(hidden).astype(jnp.float32)
        piece_out = jnp.einsum('jf,jfd->d', hidden, down_piece)
        return flat_weights[item_index] * piece_out
    items = jnp.arange(flat_experts.shape[0], dtype=jnp.int32)
    route_out = lax.map(one_route, items)
    routed = lax.optimization_barrier(jnp.sum(route_out.reshape(batch, top_count, -1), axis=1))
    mixed = (middle.astype(jnp.float32) + routed).astype(jnp.bfloat16)
    return (mixed, new_state)
```

```python
import jax
import jax.numpy as jnp
from jax import lax
from jax.sharding import Mesh
from jax.sharding import PartitionSpec as P

EXPERTS = 8
EPS = 1e-06
EP = ("zh", "zl", "x", "c")
ROW = ("zl", "x", "c")
PAIR = ("zl", "x", "c", "tp")
bf16 = jnp.bfloat16
f32 = jnp.float32


def exchange(blocks, axes):
    return lax.all_to_all(blocks, axes, split_axis=0, concat_axis=0, tiled=True)


def gathered(shard, axes, count):
    return exchange(jnp.broadcast_to(shard[None], (count, *shard.shape)), axes)


def shards(
    tokens,
    norm_gain,
    w_query,
    w_forget,
    w_input,
    forget_floor,
    head_gain,
    w_output,
    state,
    ffn_gain,
    route_experts,
    route_weights,
    w_gate,
    w_up,
    w_down,
):
    tp = lax.axis_size("tp")
    rows = lax.axis_size(ROW)
    zh = lax.axis_size("zh")
    seq, feat = tokens.shape
    width = feat * tp
    heads, head = state.shape[1], state.shape[2]
    col = w_query.shape[1]
    low = zh // tp
    here = lax.axis_index(ROW)

    w_joint = jnp.concatenate([w_query, w_forget, w_input, w_output], axis=1).T
    w_all = lax.all_gather(w_joint, "zh")
    w_in = w_all[:, : 3 * col].reshape(zh * 3 * col, feat)
    w_out = w_all[:, 3 * col :].reshape(zh * col, feat)

    tok_all = gathered(tokens, ROW, rows).reshape(rows * seq, feat).astype(f32)
    sum_sq = jnp.sum(tok_all * tok_all, axis=1)
    scaled = (tok_all * norm_gain.astype(f32)).astype(bf16)
    partial = lax.dot_general(
        scaled, w_in, (((1,), (1,)), ((), ())), preferred_element_type=f32
    )
    partial = partial.reshape(rows, seq, tp, low * 3 * col).transpose(0, 2, 1, 3)
    stat = jnp.broadcast_to(sum_sq.reshape(rows, 1, seq, 1), (rows, tp, seq, 1))
    sent = jnp.concatenate([partial, stat], axis=3).reshape(rows * tp, seq, -1)
    got = exchange(sent, PAIR).reshape(rows, tp, seq, -1).sum(axis=1)
    scale = lax.rsqrt(got[0, :, -1] / width + EPS)
    cols = got[:, :, :-1].reshape(rows, seq, low, 3, col).transpose(3, 1, 2, 0, 4)
    cols = cols.reshape(3, seq, heads, head) * scale[None, :, None, None]
    queries, fgate, inputs = cols[0], cols[1], cols[2]

    floors = forget_floor.reshape(heads, head)
    forget = floors + (1.0 - floors) * jax.nn.sigmoid(fgate)
    new_state = forget[..., None] * state + (1.0 - forget)[..., None] * inputs[:, :, None, :]
    reads = jnp.einsum(
        "bhk,bhkv->bhv", jax.nn.silu(queries), new_state, precision=lax.Precision.HIGHEST
    )
    head_sq = jnp.mean(reads * reads, axis=-1, keepdims=True)
    heads_out = (
        (reads * lax.rsqrt(head_sq + EPS) * head_gain.astype(f32))
        .reshape(seq, heads * head)
        .astype(bf16)
    )

    heads_all = gathered(heads_out, ROW, rows).reshape(rows * seq, feat)
    part_out = lax.dot_general(
        heads_all, w_out, (((1,), (1,)), ((), ())), preferred_element_type=f32
    )
    part_out = part_out.reshape(rows, seq, tp, low * col).transpose(0, 2, 1, 3)
    gain_here = lax.dynamic_index_in_dim(
        ffn_gain.astype(f32).reshape(rows, seq, feat // (rows * seq)), here, 0, False
    )
    gain_sent = jnp.broadcast_to(gain_here, (rows, tp, *gain_here.shape))
    sent = jnp.concatenate([part_out, gain_sent], axis=3).reshape(rows * tp, seq, -1)
    got = exchange(sent, PAIR).reshape(rows, tp, seq, -1)
    gain_all = got[:, :, :, low * col :].transpose(1, 0, 2, 3).reshape(tp, feat)
    mixer = got[:, :, :, : low * col].sum(axis=1).reshape(rows, seq, low, col)
    mixer = mixer.transpose(1, 2, 0, 3).reshape(seq, feat).astype(bf16)
    middle = (tokens.astype(f32) + mixer.astype(f32)).astype(bf16)

    cap = max(2, seq // 2)
    positions = jnp.arange(seq, dtype=jnp.int32)
    earlier = positions[None, :] < positions[:, None]
    same = route_experts[:, :, None, None] == route_experts[None, None, :, :]
    rank = jnp.sum(same & earlier[:, None, :, None], axis=(2, 3))
    matched = route_experts[None] == jnp.arange(EXPERTS, dtype=jnp.int32)[:, None, None]
    placed = rank[:, :, None] == jnp.arange(cap, dtype=jnp.int32)[None, None, :]
    hits = (matched[:, :, :, None] & placed[None]).astype(f32)
    chosen = jnp.sum(hits, axis=2).astype(bf16)
    weights = jnp.sum(hits * route_weights[None, :, :, None], axis=2)
    outgoing = jnp.einsum("ets,td->esd", chosen, middle, preferred_element_type=f32)
    arrived = exchange(outgoing.astype(bf16), "zh").reshape(zh * cap, feat)
    block = gathered(arrived, PAIR, rows * tp).reshape(rows, tp, zh * cap, feat)

    whole = block.transpose(0, 2, 1, 3).reshape(rows * zh * cap, width).astype(f32)
    mean_sq = jnp.mean(whole * whole, axis=1, keepdims=True)
    second = (whole * lax.rsqrt(mean_sq + EPS) * gain_all.reshape(width)).astype(bf16)
    gate = jnp.dot(second, w_gate[0], preferred_element_type=f32)
    up = jnp.dot(second, w_up[0], preferred_element_type=f32)
    hidden = (jax.nn.silu(gate) * up).astype(bf16)
    piece = jnp.dot(hidden, w_down[0], preferred_element_type=f32).astype(bf16)
    piece = piece.reshape(rows, zh * cap, tp, feat).transpose(0, 2, 1, 3)

    summed = exchange(piece.reshape(rows * tp, zh * cap, feat), PAIR)
    summed = summed.astype(f32).sum(axis=0).astype(bf16)
    returned = exchange(summed.reshape(zh, cap, feat), "zh").astype(f32)
    routed = jnp.einsum("ets,esd->td", weights, returned, precision=lax.Precision.HIGHEST)
    mixed = (middle.astype(f32) + routed).astype(bf16)
    return mixed, new_state


def solution(mesh):
    torus = Mesh(mesh.devices.reshape(8, 2, 4, 2, mesh.shape["tp"]), (*EP, "tp"))
    in_specs = (
        P(EP, "tp"),
        P("tp"),
        P("tp", EP),
        P("tp", EP),
        P("tp", EP),
        P("tp"),
        P(),
        P("tp", EP),
        P(EP, "tp", None, None),
        P("tp"),
        P(EP, None),
        P(EP, None),
        P(EP, None, "tp"),
        P(EP, None, "tp"),
        P(EP, "tp", None),
    )
    out_specs = (P(EP, "tp"), P(EP, "tp", None, None))
    return jax.shard_map(
        shards, mesh=torus, in_specs=in_specs, out_specs=out_specs, check_vma=False
    )
```

```python
import jax
import jax.numpy as jnp
from jax import lax
from jax.sharding import Mesh
from jax.sharding import PartitionSpec as P

EXPERTS = 8
EPS = 1e-06
LANES = 128
EP = ("zh", "zl", "x", "c")
ROW = ("zl", "x", "c")
PAIR = ("zl", "x", "c", "tp")
bf16 = jnp.bfloat16
f32 = jnp.float32


def exchange(blocks, axes):
    return lax.all_to_all(blocks, axes, split_axis=0, concat_axis=0, tiled=True)


def gathered(shard, axes, count):
    return exchange(jnp.broadcast_to(shard[None], (count, *shard.shape)), axes)


def shards(
    tokens,
    norm_gain,
    w_query,
    w_forget,
    w_input,
    forget_floor,
    head_gain,
    w_output,
    state,
    ffn_gain,
    route_experts,
    route_weights,
    w_gate,
    w_up,
    w_down,
):
    tp = lax.axis_size("tp")
    rows = lax.axis_size(ROW)
    zh = lax.axis_size("zh")
    seq, feat = tokens.shape
    width = feat * tp
    heads, head = state.shape[1], state.shape[2]
    col = w_query.shape[1]
    low = zh // tp
    here = lax.axis_index(ROW)

    w_joint = jnp.concatenate([w_query, w_forget, w_input, w_output], axis=1).T
    w_all = gathered(w_joint, "zh", zh)

    tok_all = tokens
    for axis in reversed(ROW):
        tok_all = lax.all_gather(tok_all, axis, tiled=True)
    mine = jnp.concatenate([w_gate[0].T, w_up[0].T, w_down[0]], axis=0)
    other = lax.ppermute(mine, "c", [(0, 1), (1, 0)])
    w_all, tok_all, mine, other = lax.optimization_barrier((w_all, tok_all, mine, other))
    w_in = w_all[:, : 3 * col].reshape(tp, low * 3 * col, feat)
    w_out = w_all[:, 3 * col :].reshape(tp, low * col, feat)

    tok_all = tok_all.astype(f32)
    sum_sq = jnp.sum(tok_all * tok_all, axis=1)
    scaled = (tok_all * norm_gain.astype(f32)).astype(bf16)
    partial = jnp.einsum("td,pcd->tpc", scaled, w_in, preferred_element_type=f32)
    partial = partial.reshape(rows, seq, tp, low * 3 * col).transpose(0, 2, 1, 3)
    used = low * 3 * col
    stat = jnp.broadcast_to(sum_sq.reshape(rows, 1, seq, 1), (rows, tp, seq, LANES - used))
    sent = jnp.concatenate([partial, stat], axis=3).reshape(rows * tp, seq, LANES)
    got = exchange(sent, PAIR).reshape(rows, tp, seq, LANES).sum(axis=1)
    scale = lax.rsqrt(got[0, :, LANES - 1] / width + EPS)
    cols = got[:, :, :used].reshape(rows, seq, low, 3, col).transpose(3, 1, 2, 0, 4)
    cols = cols.reshape(3, seq, heads, head) * scale[None, :, None, None]
    queries, fgate, inputs = cols[0], cols[1], cols[2]

    floors = forget_floor.reshape(heads, head)
    forget = floors + (1.0 - floors) * jax.nn.sigmoid(fgate)
    new_state = forget[..., None] * state + (1.0 - forget)[..., None] * inputs[:, :, None, :]
    reads = jnp.einsum(
        "bhk,bhkv->bhv", jax.nn.silu(queries), new_state, precision=lax.Precision.HIGHEST
    )
    head_sq = jnp.mean(reads * reads, axis=-1, keepdims=True)
    heads_out = (
        (reads * lax.rsqrt(head_sq + EPS) * head_gain.astype(f32))
        .reshape(seq, heads * head)
        .astype(bf16)
    )

    heads_all = gathered(heads_out, ROW, rows).reshape(rows * seq, feat)
    part_out = jnp.einsum("td,pcd->tpc", heads_all, w_out, preferred_element_type=f32)
    part_out = part_out.reshape(rows, seq, tp, low * col).transpose(0, 2, 1, 3)
    share = feat // (rows * seq)
    gain_here = lax.dynamic_index_in_dim(
        ffn_gain.astype(f32).reshape(rows, seq, share), here, 0, False
    )
    gain_sent = jnp.broadcast_to(gain_here, (rows, tp, seq, share))
    rest = jnp.zeros((rows, tp, seq, LANES - low * col - share), f32)
    sent = jnp.concatenate([part_out, gain_sent, rest], axis=3).reshape(rows * tp, seq, LANES)
    got = exchange(sent, PAIR).reshape(rows, tp, seq, LANES)
    gain_all = got[:, :, :, low * col : low * col + share].transpose(1, 0, 2, 3).reshape(width)
    mixer = got[:, :, :, : low * col].sum(axis=1).reshape(rows, seq, low, col)
    mixer = mixer.transpose(1, 2, 0, 3).reshape(seq, feat).astype(bf16)
    middle = (tokens.astype(f32) + mixer.astype(f32)).astype(bf16)

    cap = max(2, seq // 2)
    positions = jnp.arange(seq, dtype=jnp.int32)
    earlier = positions[None, :] < positions[:, None]
    same = route_experts[:, :, None, None] == route_experts[None, None, :, :]
    rank = jnp.sum(same & earlier[:, None, :, None], axis=(2, 3))
    matched = route_experts[None] == jnp.arange(EXPERTS, dtype=jnp.int32)[:, None, None]
    placed = rank[:, :, None] == jnp.arange(cap, dtype=jnp.int32)[None, None, :]
    hits = (matched[:, :, :, None] & placed[None]).astype(f32)
    chosen = jnp.sum(hits, axis=2).astype(bf16)
    weights = jnp.sum(hits * route_weights[None, :, :, None], axis=2)
    outgoing = jnp.einsum("ets,td->esd", chosen, middle, preferred_element_type=f32)
    arrived = exchange(outgoing.astype(bf16), "zh").transpose(1, 0, 2)
    zl, x, c = (lax.axis_size(a) for a in ROW)
    sent = jnp.broadcast_to(arrived[None, None, :, None], (zl, x, c, tp, zh, feat))
    block = exchange(sent.reshape(rows * tp, zh, feat), PAIR).reshape(rows, tp, zh, feat)

    whole = block.transpose(0, 2, 1, 3).reshape(rows * zh, width).astype(f32)
    mean_sq = jnp.mean(whole * whole, axis=1, keepdims=True)
    second = (whole * lax.rsqrt(mean_sq + EPS) * gain_all).astype(bf16)
    units = w_gate.shape[2]
    piece = jnp.zeros((rows * zh, width), f32)
    for w in (mine, other):
        gate = jnp.einsum("rd,fd->rf", second, w[:units], preferred_element_type=f32)
        up = jnp.einsum("rd,fd->rf", second, w[units : 2 * units], preferred_element_type=f32)
        hidden = (jax.nn.silu(gate) * up).astype(bf16)
        piece = piece + jnp.dot(hidden, w[2 * units :], preferred_element_type=f32)
    piece = piece.astype(bf16).reshape(rows, zh, tp, feat).transpose(0, 2, 1, 3)

    summed = exchange(piece.reshape(rows * tp, zh, feat), PAIR).astype(f32)
    summed = summed.reshape(zl, x, c, tp, zh, feat).sum(axis=(0, 1, 3)).astype(bf16)
    returned = exchange(summed.transpose(1, 0, 2), "zh").astype(f32)
    routed = jnp.einsum("ets,esd->td", weights, returned, precision=lax.Precision.HIGHEST)
    mixed = (middle.astype(f32) + routed).astype(bf16)
    return mixed, new_state


def solution(mesh):
    torus = Mesh(mesh.devices.reshape(8, 2, 4, 2, mesh.shape["tp"]), (*EP, "tp"))
    in_specs = (
        P(EP, "tp"),
        P("tp"),
        P("tp", EP),
        P("tp", EP),
        P("tp", EP),
        P("tp"),
        P(),
        P("tp", EP),
        P(EP, "tp", None, None),
        P("tp"),
        P(EP, None),
        P(EP, None),
        P(EP, None, "tp"),
        P(EP, None, "tp"),
        P(EP, "tp", None),
    )
    out_specs = (P(EP, "tp"), P(EP, "tp", None, None))
    return jax.shard_map(
        shards, mesh=torus, in_specs=in_specs, out_specs=out_specs, check_vma=False
    )
```

```python
import jax
import jax.numpy as jnp
from jax import lax
from jax.experimental import pallas as pl
from jax.experimental.pallas import tpu as pltpu
from jax.sharding import Mesh
from jax.sharding import PartitionSpec as P

EXPERTS = 8
EPS = 1e-06
LANES = 128
EP = ("zh", "zl", "x", "c")
ROW = ("zl", "x", "c")
PAIR = ("zl", "x", "c", "tp")
bf16 = jnp.bfloat16
f32 = jnp.float32


def exchange(blocks, axes):
    return lax.all_to_all(blocks, axes, split_axis=0, concat_axis=0, tiled=True)


def gathered(shard, axes, count):
    return exchange(jnp.broadcast_to(shard[None], (count, *shard.shape)), axes)


def slot_hits(experts, cap):
    positions = jnp.arange(experts.shape[1], dtype=jnp.int32)
    earlier = positions[None, :] < positions[:, None]
    same = experts[:, :, :, None, None] == experts[:, None, None, :, :]
    rank = jnp.sum(same & earlier[None, :, None, :, None], axis=(3, 4))
    matched = experts[None] == jnp.arange(EXPERTS, dtype=jnp.int32)[:, None, None, None]
    placed = rank[..., None] == jnp.arange(cap, dtype=jnp.int32)
    return (matched[..., None] & placed[None]).astype(f32)


def chosen_slots(experts, cap):
    return jnp.sum(slot_hits(experts, cap), axis=3)


def recurrence_kernel(
    width, got_ref, state_ref, floor_ref, gain_ref, out_ref, forget_ref, input_ref, held, sem
):
    copy = pltpu.make_async_copy(state_ref, held, sem)
    copy.start()
    sources, parts, seq, lanes = got_ref.shape
    heads = forget_ref.shape[0]
    half = sources // 2
    col = lanes // half
    summed = []
    for s in range(half):
        both = []
        for source in (s, s + half):
            block = got_ref[source, 0]
            for part in range(1, parts):
                block = block + got_ref[source, part]
            both.append(block)
        summed.append(jnp.concatenate(both, axis=0))
    stat = summed[0][:seq, lanes - 1 :]
    scale = lax.rsqrt(stat / width + EPS)
    scale = jnp.concatenate([scale, scale], axis=0)
    lane = lax.broadcasted_iota(jnp.int32, (2 * seq, lanes), 1) // col
    first = lax.broadcasted_iota(jnp.int32, (2 * seq, lanes), 0) < seq

    def columns(low, which):
        total = jnp.zeros((2 * seq, lanes), f32)
        at = (low * 3 + which) * col
        for s in range(half):
            moved = pltpu.roll(summed[s], (s * col - at) % lanes, 1)
            total = jnp.where(lane == s, moved, total)
        return total * scale

    rows = []
    for low in range(heads // 2):
        query, gate, value = (columns(low, which) for which in range(3))
        floor = jnp.where(first, floor_ref[2 * low][None, :], floor_ref[2 * low + 1][None, :])
        forget = floor + (1.0 - floor) / (1.0 + jnp.exp(-gate))
        query = query / (1.0 + jnp.exp(-query))
        for k in range(2):
            forget_ref[2 * low + k] = forget[k * seq : (k + 1) * seq]
            input_ref[2 * low + k] = value[k * seq : (k + 1) * seq]
        fresh = jnp.sum(query * (1.0 - forget), axis=1, keepdims=True)
        rows.append((fresh * value, (query * forget).T))
    copy.wait()
    gain = gain_ref[...].astype(f32)
    for low in range(heads // 2):
        fresh, kept = rows[low]
        old = []
        for k in range(2):
            for t in range(seq):
                r = k * seq + t
                old.append(
                    jnp.sum(kept[:, r : r + 1] * held[t, 2 * low + k], axis=0, keepdims=True)
                )
        reads = fresh + jnp.concatenate(old, axis=0)
        mean_sq = jnp.mean(reads * reads, axis=1, keepdims=True)
        normed = (reads * lax.rsqrt(mean_sq + EPS) * gain).astype(bf16)
        for k in range(2):
            head = 2 * low + k
            block = normed[k * seq : (k + 1) * seq]
            for n in range(out_ref.shape[0]):
                out_ref[n, :, head * lanes : (head + 1) * lanes] = block


def recurrence(width, got, state, floors, gain):
    sources, _, seq, lanes = got.shape
    heads = state.shape[1]
    return pl.pallas_call(
        lambda *refs: recurrence_kernel(width, *refs),
        out_shape=(
            jax.ShapeDtypeStruct((sources, seq, heads * lanes), bf16),
            jax.ShapeDtypeStruct((heads, seq, lanes), f32),
            jax.ShapeDtypeStruct((heads, seq, lanes), f32),
        ),
        in_specs=[
            pl.BlockSpec(memory_space=pltpu.VMEM),
            pl.BlockSpec(memory_space=pl.ANY),
            pl.BlockSpec(memory_space=pltpu.VMEM),
            pl.BlockSpec(memory_space=pltpu.VMEM),
        ],
        out_specs=tuple(pl.BlockSpec(memory_space=pltpu.VMEM) for _ in range(3)),
        scratch_shapes=[pltpu.VMEM(state.shape, f32), pltpu.SemaphoreType.DMA],
        name="recurrence",
    )(got, state, floors, gain)


def shards(
    tokens,
    norm_gain,
    w_query,
    w_forget,
    w_input,
    forget_floor,
    head_gain,
    w_output,
    state,
    ffn_gain,
    route_experts,
    route_weights,
    w_gate,
    w_up,
    w_down,
):
    tp = lax.axis_size("tp")
    rows = lax.axis_size(ROW)
    zh = lax.axis_size("zh")
    seq, feat = tokens.shape
    width = feat * tp
    heads, head = state.shape[1], state.shape[2]
    col = w_query.shape[1]
    low = zh // tp
    here = lax.axis_index(ROW)
    zl, x, c = (lax.axis_size(a) for a in ROW)
    cap = max(2, seq // 2)

    w_joint = jnp.concatenate([w_query, w_forget, w_input, w_output], axis=1).T
    w_all = gathered(w_joint, "zh", zh)

    routes = jnp.pad(route_experts.astype(bf16), ((0, 0), (0, feat - route_experts.shape[1])))
    all_rows = jnp.concatenate([tokens, routes], axis=0)
    for axis in reversed(ROW):
        all_rows = lax.all_gather(all_rows, axis, tiled=True)
    w_all, all_rows = lax.optimization_barrier((w_all, all_rows))
    all_rows = all_rows.reshape(rows, 2, seq, feat)
    tok_all = all_rows[:, 0].reshape(rows * seq, feat)
    experts_all = all_rows[:, 1, :, : route_experts.shape[1]].astype(jnp.int32)
    w_in = w_all[:, : 3 * col].reshape(tp, low * 3 * col, feat)
    w_out = w_all[:, 3 * col :].reshape(tp, low * col, feat)

    tok_all = tok_all.astype(f32)
    sum_sq = jnp.sum(tok_all * tok_all, axis=1)
    scaled = (tok_all * norm_gain.astype(f32)).astype(bf16)
    partial = jnp.einsum("td,pcd->tpc", scaled, w_in, preferred_element_type=f32)
    partial = partial.reshape(rows, seq, tp, low * 3 * col).transpose(0, 2, 1, 3)
    used = low * 3 * col
    share = feat // (rows * seq)
    gain_here = lax.dynamic_index_in_dim(
        ffn_gain.astype(f32).reshape(rows, seq, share), here, 0, False
    )
    gain_sent = jnp.broadcast_to(gain_here, (rows, tp, seq, share))
    stat = jnp.broadcast_to(sum_sq.reshape(rows, 1, seq, 1), (rows, tp, seq, LANES - used - share))
    sent = jnp.concatenate([partial, gain_sent, stat], axis=3).reshape(rows * tp, seq, LANES)
    got = exchange(sent, PAIR).reshape(rows, tp, seq, LANES)

    heads_sent, forget, inputs = recurrence(
        width, got, state, forget_floor.reshape(heads, head), head_gain.reshape(1, head)
    )
    forget, inputs = forget.transpose(1, 0, 2), inputs.transpose(1, 0, 2)
    new_state = forget[..., None] * state + (1.0 - forget)[..., None] * inputs[:, :, None, :]

    quarter = rows // tp
    sel = chosen_slots(experts_all, cap).reshape(EXPERTS, tp, quarter, seq, cap)
    sel = sel.transpose(0, 1, 4, 2, 3)
    eye = jnp.eye(rows, dtype=f32).reshape(tp, quarter, rows)
    sel = sel[:, :, :, :, None, :] * eye[None, :, None, :, :, None]
    sel = sel.reshape(EXPERTS * rows * cap, rows * seq).astype(bf16)

    heads_all = exchange(heads_sent, ROW).reshape(rows * seq, feat)
    part_out = jnp.einsum("td,pcd->tpc", heads_all, w_out, preferred_element_type=f32)
    residual = lax.dynamic_index_in_dim(
        tok_all.reshape(rows * seq, low, rows, col), here, 2, False
    ).reshape(rows * seq, 1, low * col)
    own = (jnp.arange(tp) == lax.axis_index("tp"))[None, :, None]
    with_tok = (part_out + jnp.where(own, residual, 0.0)).reshape(rows * seq, tp * low * col)

    outgoing = jnp.dot(sel, with_tok.astype(bf16), preferred_element_type=f32).astype(bf16)
    arrived = exchange(outgoing.reshape(zh * tp, cap * quarter, LANES), ("zh", "tp"))
    arrived = arrived.astype(f32).reshape(zh, tp, cap, quarter, LANES).sum(axis=1).astype(bf16)
    arrived = arrived.transpose(1, 2, 0, 3).reshape(cap, quarter * zh, LANES)
    sent = jnp.broadcast_to(
        arrived[None, None, :, None], (zl, x, c, tp, quarter * zh, LANES)
    ).reshape(rows * tp, quarter * zh, LANES)
    block = exchange(sent, PAIR).reshape(rows, tp, quarter * zh, LANES)

    def ordered(w):
        return w.reshape(zh, rows, col, -1).transpose(1, 0, 2, 3).reshape(width, -1)

    pair = lambda w: lax.ppermute(w, "c", [(0, 1), (1, 0)])
    gate_up = jnp.concatenate([ordered(w_gate[0]), ordered(w_up[0])], axis=1)
    down = w_down[0]
    gain_all = got[:, :, :, used : used + share].transpose(1, 0, 2, 3)
    gain_all = ordered(gain_all.reshape(width, 1)).reshape(width)

    whole = block.transpose(1, 2, 0, 3).reshape(rows * zh, width).astype(f32)
    mean_sq = jnp.mean(whole * whole, axis=1, keepdims=True)
    second = (whole * lax.rsqrt(mean_sq + EPS) * gain_all).astype(bf16)
    units = w_gate.shape[2]
    piece = jnp.zeros((rows * zh, width), f32)
    for w, w_d in ((gate_up, down), (pair(gate_up), pair(down))):
        both = jnp.dot(second, w, preferred_element_type=f32)
        hidden = (jax.nn.silu(both[:, :units]) * both[:, units:]).astype(bf16)
        piece = piece + jnp.dot(hidden, w_d, preferred_element_type=f32)
    piece = piece.astype(bf16).reshape(rows, zh, tp, feat).transpose(0, 2, 1, 3)

    rider = part_out.reshape(rows, seq, tp, low * col).transpose(0, 2, 1, 3)
    rider = jnp.pad(rider.astype(bf16), ((0, 0), (0, 0), (0, zh - seq), (0, LANES - low * col)))
    back = jnp.concatenate([piece, rider], axis=3).reshape(rows * tp, zh, feat + LANES)
    back = exchange(back, PAIR).astype(f32)
    summed = back[:, :, :feat].reshape(zl, x, c, tp, zh, feat).sum(axis=(0, 1, 3)).astype(bf16)
    returned = exchange(summed.transpose(1, 0, 2), "zh").astype(f32)
    mixer = back[:, :seq, feat : feat + low * col].reshape(rows, tp, seq, low, col).sum(axis=1)
    mixer = mixer.transpose(1, 2, 0, 3).reshape(seq, feat).astype(bf16)
    middle = (tokens.astype(f32) + mixer.astype(f32)).astype(bf16)

    hits = slot_hits(route_experts[None], cap)[:, 0]
    weights = jnp.sum(hits * route_weights[None, :, :, None], axis=2)
    routed = jnp.einsum("ets,esd->td", weights, returned, precision=lax.Precision.HIGHEST)
    mixed = (middle.astype(f32) + routed).astype(bf16)
    return mixed, new_state


def solution(mesh):
    torus = Mesh(mesh.devices.reshape(8, 2, 4, 2, mesh.shape["tp"]), (*EP, "tp"))
    in_specs = (
        P(EP, "tp"),
        P("tp"),
        P("tp", EP),
        P("tp", EP),
        P("tp", EP),
        P("tp"),
        P(),
        P("tp", EP),
        P(EP, "tp", None, None),
        P("tp"),
        P(EP, None),
        P(EP, None),
        P(EP, None, "tp"),
        P(EP, None, "tp"),
        P(EP, "tp", None),
    )
    out_specs = (P(EP, "tp"), P(EP, "tp", None, None))
    return jax.shard_map(
        shards, mesh=torus, in_specs=in_specs, out_specs=out_specs, check_vma=False
    )
```

```python
import jax
import jax.numpy as jnp
from jax import lax
from jax.experimental import pallas as pl
from jax.experimental.pallas import tpu as pltpu
from jax.sharding import Mesh
from jax.sharding import PartitionSpec as P

EXPERTS = 8
EPS = 1e-06
LANES = 128
EP = ("zh", "zl", "xh", "xl", "c")
ROW = ("zl", "xh", "xl", "c")
PAIR = (*ROW, "tp")
GATHER = ("zl", "xl", "xh", "c")
bf16 = jnp.bfloat16
f32 = jnp.float32


def exchange(blocks, axes):
    return lax.all_to_all(blocks, axes, split_axis=0, concat_axis=0, tiled=True)


def gathered(shard, axes, count):
    return exchange(jnp.broadcast_to(shard[None], (count, *shard.shape)), axes)


def slot_hits(experts, cap):
    positions = jnp.arange(experts.shape[1], dtype=jnp.int32)
    earlier = positions[None, :] < positions[:, None]
    same = experts[:, :, :, None, None] == experts[:, None, None, :, :]
    rank = jnp.sum(same & earlier[None, :, None, :, None], axis=(3, 4))
    matched = experts[None] == jnp.arange(EXPERTS, dtype=jnp.int32)[:, None, None, None]
    placed = rank[..., None] == jnp.arange(cap, dtype=jnp.int32)
    return (matched[..., None] & placed[None]).astype(f32)


def chosen_slots(experts, cap):
    return jnp.sum(slot_hits(experts, cap), axis=3)


def resident(value):
    return pltpu.with_memory_space_constraint(value, pltpu.VMEM)


def recurrence_kernel(
    width, got_ref, state_ref, floor_ref, gain_ref, out_ref, forget_ref, input_ref, held, sem
):
    copy = pltpu.make_async_copy(state_ref, held, sem)
    copy.start()
    sources, parts, seq, lanes = got_ref.shape
    heads = forget_ref.shape[0]
    half = sources // 2
    col = lanes // half
    summed = []
    for s in range(half):
        both = []
        for source in (s, s + half):
            block = got_ref[source, 0]
            for part in range(1, parts):
                block = block + got_ref[source, part]
            both.append(block)
        summed.append(jnp.concatenate(both, axis=0))
    stat = summed[0][:seq, lanes - 1 :]
    scale = lax.rsqrt(stat / width + EPS)
    scale = jnp.concatenate([scale, scale], axis=0)
    lane = lax.broadcasted_iota(jnp.int32, (2 * seq, lanes), 1) // col
    first = lax.broadcasted_iota(jnp.int32, (2 * seq, lanes), 0) < seq

    def columns(low, which):
        total = jnp.zeros((2 * seq, lanes), f32)
        at = (low * 3 + which) * col
        for s in range(half):
            moved = pltpu.roll(summed[s], (s * col - at) % lanes, 1)
            total = jnp.where(lane == s, moved, total)
        return total * scale

    rows = []
    for low in range(heads // 2):
        query, gate, value = (columns(low, which) for which in range(3))
        floor = jnp.where(first, floor_ref[2 * low][None, :], floor_ref[2 * low + 1][None, :])
        forget = floor + (1.0 - floor) / (1.0 + jnp.exp(-gate))
        query = query / (1.0 + jnp.exp(-query))
        for k in range(2):
            forget_ref[2 * low + k] = forget[k * seq : (k + 1) * seq]
            input_ref[2 * low + k] = value[k * seq : (k + 1) * seq]
        fresh = jnp.sum(query * (1.0 - forget), axis=1, keepdims=True)
        rows.append((fresh * value, (query * forget).T))
    copy.wait()
    gain = gain_ref[...].astype(f32)
    for low in range(heads // 2):
        fresh, kept = rows[low]
        old = []
        for k in range(2):
            for t in range(seq):
                r = k * seq + t
                old.append(
                    jnp.sum(kept[:, r : r + 1] * held[t, 2 * low + k], axis=0, keepdims=True)
                )
        reads = fresh + jnp.concatenate(old, axis=0)
        mean_sq = jnp.mean(reads * reads, axis=1, keepdims=True)
        normed = (reads * lax.rsqrt(mean_sq + EPS) * gain).astype(bf16)
        for k in range(2):
            head = 2 * low + k
            block = normed[k * seq : (k + 1) * seq]
            for n in range(out_ref.shape[0]):
                out_ref[n, :, head * lanes : (head + 1) * lanes] = block


def recurrence(width, got, state, floors, gain):
    sources, _, seq, lanes = got.shape
    heads = state.shape[1]
    return pl.pallas_call(
        lambda *refs: recurrence_kernel(width, *refs),
        out_shape=(
            jax.ShapeDtypeStruct((sources, seq, heads * lanes), bf16),
            jax.ShapeDtypeStruct((heads, seq, lanes), f32),
            jax.ShapeDtypeStruct((heads, seq, lanes), f32),
        ),
        in_specs=[
            pl.BlockSpec(memory_space=pltpu.VMEM),
            pl.BlockSpec(memory_space=pl.ANY),
            pl.BlockSpec(memory_space=pltpu.VMEM),
            pl.BlockSpec(memory_space=pltpu.VMEM),
        ],
        out_specs=tuple(pl.BlockSpec(memory_space=pltpu.VMEM) for _ in range(3)),
        scratch_shapes=[pltpu.VMEM(state.shape, f32), pltpu.SemaphoreType.DMA],
        name="recurrence",
    )(resident(got), state, floors, gain)


def experts_kernel(
    rows_v, gain_ref, gu0_ref, down0_ref, gu1_ref, down1_ref, rider_ref, out_ref,
    second, gu_v, down_v, out_v, sems, out_sems,
):
    copies = [
        pltpu.make_async_copy(src, dst, sems.at[n])
        for n, (src, dst) in enumerate(
            (
                (gu0_ref, gu_v.at[0]),
                (gu1_ref, gu_v.at[1]),
                (down0_ref, down_v.at[0]),
                (down1_ref, down_v.at[1]),
            )
        )
    ]
    for copy in copies:
        copy.start()
    sources, parts, height, lanes = rows_v.shape
    count = parts * height
    zh, feat = out_v.shape[2], out_v.shape[3] - lanes
    out_v[:, :, :, feat:] = rider_ref[...]
    total = jnp.zeros((count, lanes), f32)
    for n in range(sources):
        block = rows_v[n].reshape(count, lanes).astype(f32)
        total = total + block * block
    scale = lax.rsqrt(jnp.sum(total, axis=1, keepdims=True) / (sources * lanes) + EPS)
    for n in range(sources):
        block = rows_v[n].reshape(count, lanes).astype(f32)
        second[:, n * lanes : (n + 1) * lanes] = (block * scale * gain_ref[n]).astype(bf16)
    copies[0].wait()
    copies[1].wait()
    hidden = []
    for k in range(2):
        both = jnp.dot(second[...], gu_v[k], preferred_element_type=f32)
        gate = both[:, :lanes]
        hidden.append((gate / (1.0 + jnp.exp(-gate)) * both[:, lanes:]).astype(bf16))
    copies[2].wait()
    copies[3].wait()
    outs = []
    for part in range(parts):
        at = slice(part * feat, (part + 1) * feat)
        piece = jnp.dot(hidden[0], down_v[0, :, at], preferred_element_type=f32)
        piece = piece + jnp.dot(hidden[1], down_v[1, :, at], preferred_element_type=f32)
        out_v[:, part, :, :feat] = piece.astype(bf16).reshape(count // zh, zh, feat)
        outs.append(pltpu.make_async_copy(out_v.at[:, part], out_ref.at[:, part], out_sems.at[part]))
        outs[-1].start()
    for copy in outs:
        copy.wait()


def experts(block, gain, weights_of, rider):
    sources, parts, height, lanes = block.shape
    (gate_up, down), (gate_up_1, down_1) = weights_of
    zh = rider.shape[2]
    feat = gate_up.shape[0] // parts
    count = parts * height
    whole = (count // zh, parts, zh, feat + lanes)
    anywhere = pl.BlockSpec(memory_space=pl.ANY)
    vmem = pl.BlockSpec(memory_space=pltpu.VMEM)
    return pl.pallas_call(
        experts_kernel,
        out_shape=jax.ShapeDtypeStruct(whole, bf16),
        in_specs=[vmem, vmem, anywhere, anywhere, anywhere, anywhere, vmem],
        out_specs=anywhere,
        scratch_shapes=[
            pltpu.VMEM((count, gate_up.shape[0]), bf16),
            pltpu.VMEM((2, *gate_up.shape), bf16),
            pltpu.VMEM((2, *down.shape), bf16),
            pltpu.VMEM(whole, bf16),
            pltpu.SemaphoreType.DMA((4,)),
            pltpu.SemaphoreType.DMA((parts,)),
        ],
        name="experts",
    )(resident(block), gain, gate_up, down, gate_up_1, down_1, rider)


def shards(
    tokens,
    norm_gain,
    w_query,
    w_forget,
    w_input,
    forget_floor,
    head_gain,
    w_output,
    state,
    ffn_gain,
    route_experts,
    route_weights,
    w_gate,
    w_up,
    w_down,
):
    tp = lax.axis_size("tp")
    rows = lax.axis_size(ROW)
    zh = lax.axis_size("zh")
    seq, feat = tokens.shape
    width = feat * tp
    heads, head = state.shape[1], state.shape[2]
    col = w_query.shape[1]
    low = zh // tp
    here = lax.axis_index(ROW)
    c = lax.axis_size("c")
    chips = rows // c
    cap = max(2, seq // 2)

    w_joint = jnp.concatenate([w_query, w_forget, w_input, w_output], axis=1).T
    w_all = gathered(w_joint, "zh", zh)

    routes = jnp.pad(route_experts.astype(bf16), ((0, 0), (0, feat - route_experts.shape[1])))
    all_rows = jnp.concatenate([tokens, routes], axis=0)
    for axis in GATHER:
        all_rows = lax.all_gather(all_rows, axis, tiled=True)

    all_rows = all_rows.reshape(2, 2, 2, 2, 2, seq, feat)
    order = tuple(GATHER[::-1].index(axis) for axis in ROW)
    all_rows = all_rows.transpose(*order, 4, 5, 6).reshape(rows, 2, seq, feat)
    experts_all = all_rows[:, 1, :, : route_experts.shape[1]].astype(jnp.int32)
    w_all, tok_all = lax.optimization_barrier((w_all, all_rows[:, 0].reshape(rows * seq, feat)))
    w_in = w_all[:, : 3 * col].reshape(tp, low * 3 * col, feat)
    w_out = w_all[:, 3 * col :].reshape(tp, low * col, feat)

    tok_all = tok_all.astype(f32)
    sum_sq = jnp.sum(tok_all * tok_all, axis=1)
    scaled = (tok_all * norm_gain.astype(f32)).astype(bf16)
    partial = jnp.einsum("td,pcd->tpc", scaled, w_in, preferred_element_type=f32)
    partial = partial.reshape(rows, seq, tp, low * 3 * col).transpose(0, 2, 1, 3)
    used = low * 3 * col
    share = feat // (rows * seq)
    gain_here = lax.dynamic_index_in_dim(
        ffn_gain.astype(f32).reshape(rows, seq, share), here, 0, False
    )
    gain_sent = jnp.broadcast_to(gain_here, (rows, tp, seq, share))
    stat = jnp.broadcast_to(sum_sq.reshape(rows, 1, seq, 1), (rows, tp, seq, LANES - used - share))
    sent = jnp.concatenate([partial, gain_sent, stat], axis=3).reshape(rows * tp, seq, LANES)
    got = exchange(sent, PAIR).reshape(rows, tp, seq, LANES)

    heads_sent, forget, inputs = recurrence(
        width, got, state, forget_floor.reshape(heads, head), head_gain.reshape(1, head)
    )
    forget, inputs = forget.transpose(1, 0, 2), inputs.transpose(1, 0, 2)
    new_state = forget[..., None] * state + (1.0 - forget)[..., None] * inputs[:, :, None, :]

    quarter = rows // tp
    sel = chosen_slots(experts_all, cap).reshape(EXPERTS, tp, quarter, seq, cap)
    sel = sel.transpose(0, 1, 4, 2, 3)
    eye = jnp.eye(rows, dtype=f32).reshape(tp, quarter, rows)
    sel = sel[:, :, :, :, None, :] * eye[None, :, None, :, :, None]
    sel = sel.reshape(EXPERTS * rows * cap, rows * seq).astype(bf16)

    heads_all = exchange(heads_sent, ROW).reshape(rows * seq, feat)
    part_out = jnp.einsum("td,pcd->tpc", heads_all, w_out, preferred_element_type=f32)
    residual = lax.dynamic_index_in_dim(
        tok_all.reshape(rows * seq, low, rows, col), here, 2, False
    ).reshape(rows * seq, 1, low * col)
    own = (jnp.arange(tp) == lax.axis_index("tp"))[None, :, None]
    with_tok = (part_out + jnp.where(own, residual, 0.0)).reshape(rows * seq, tp * low * col)

    outgoing = jnp.dot(sel, with_tok.astype(bf16), preferred_element_type=f32).astype(bf16)
    arrived = exchange(outgoing.reshape(zh * tp, cap * quarter, LANES), ("zh", "tp"))
    arrived = arrived.astype(f32).reshape(zh, tp, cap, quarter, LANES).sum(axis=1).astype(bf16)
    arrived = arrived.transpose(1, 2, 0, 3).reshape(cap, quarter * zh, LANES)
    sent = jnp.broadcast_to(
        arrived[None, :, None], (chips, c, tp, quarter * zh, LANES)
    ).reshape(rows * tp, quarter * zh, LANES)
    block = exchange(sent, PAIR).reshape(rows, tp, quarter * zh, LANES)

    def ordered(w):
        return w.reshape(zh, rows, col, -1).transpose(1, 0, 2, 3).reshape(width, -1)

    units = w_gate.shape[2]
    fill = ((0, 0), (0, LANES - units))
    gate_up = jnp.concatenate(
        [jnp.pad(ordered(w_gate[0]), fill), jnp.pad(ordered(w_up[0]), fill)], axis=1
    )
    down = jnp.pad(w_down[0], fill[::-1])
    weights_of = [(gate_up, down), tuple(lax.ppermute(w, "c", [(0, 1), (1, 0)]) for w in (gate_up, down))]

    gain_all = got[:, :, :, used : used + share].transpose(1, 0, 2, 3)
    gain_all = ordered(gain_all.reshape(width, 1)).reshape(rows, 1, LANES)
    rider = part_out.reshape(rows, seq, tp, low * col).transpose(0, 2, 1, 3)
    rider = jnp.pad(rider.astype(bf16), ((0, 0), (0, 0), (0, zh - seq), (0, LANES - low * col)))
    back = experts(block, gain_all, weights_of, rider)
    back = back.reshape(rows * tp, zh, feat + LANES)
    back = exchange(back, PAIR).astype(f32)
    summed = back[:, :, :feat].reshape(chips, c, tp, zh, feat).sum(axis=(0, 2)).astype(bf16)
    returned = exchange(summed.transpose(1, 0, 2), "zh").astype(f32)
    mixer = back[:, :seq, feat : feat + low * col].reshape(rows, tp, seq, low, col).sum(axis=1)
    mixer = mixer.transpose(1, 2, 0, 3).reshape(seq, feat).astype(bf16)
    middle = (tokens.astype(f32) + mixer.astype(f32)).astype(bf16)

    hits = slot_hits(route_experts[None], cap)[:, 0]
    weights = jnp.sum(hits * route_weights[None, :, :, None], axis=2)
    routed = jnp.einsum("ets,esd->td", weights, returned, precision=lax.Precision.HIGHEST)
    mixed = (middle.astype(f32) + routed).astype(bf16)
    return mixed, new_state


def solution(mesh):
    torus = Mesh(mesh.devices.reshape(8, 2, 2, 2, 2, mesh.shape["tp"]), (*EP, "tp"))
    in_specs = (
        P(EP, "tp"),
        P("tp"),
        P("tp", EP),
        P("tp", EP),
        P("tp", EP),
        P("tp"),
        P(),
        P("tp", EP),
        P(EP, "tp", None, None),
        P("tp"),
        P(EP, None),
        P(EP, None),
        P(EP, None, "tp"),
        P(EP, None, "tp"),
        P(EP, "tp", None),
    )
    out_specs = (P(EP, "tp"), P(EP, "tp", None, None))
    return jax.shard_map(
        shards, mesh=torus, in_specs=in_specs, out_specs=out_specs, check_vma=False
    )
```

```python
import jax
import jax.numpy as jnp
from jax import lax
from jax.experimental import pallas as pl
from jax.experimental.pallas import tpu as pltpu
from jax.sharding import Mesh
from jax.sharding import PartitionSpec as P

EXPERTS = 8
EPS = 1e-06
LANES = 128
ZH = ("za", "zm")
EP = (*ZH, "zl", "xh", "xl", "c")
ROW = ("zl", "xh", "xl", "c")
PAIR = (*ROW, "tp")
WIDE = ("zm", *ROW)
GATHER = ("zl", "zm", "xl", "xh", "c")
bf16 = jnp.bfloat16
f32 = jnp.float32


def exchange(blocks, axes):
    return lax.all_to_all(blocks, axes, split_axis=0, concat_axis=0, tiled=True)


def gathered(shard, axes, count):
    return exchange(jnp.broadcast_to(shard[None], (count, *shard.shape)), axes)


def slot_hits(experts, cap):
    positions = jnp.arange(experts.shape[1], dtype=jnp.int32)
    earlier = positions[None, :] < positions[:, None]
    same = experts[:, :, :, None, None] == experts[:, None, None, :, :]
    rank = jnp.sum(same & earlier[None, :, None, :, None], axis=(3, 4))
    matched = experts[None] == jnp.arange(EXPERTS, dtype=jnp.int32)[:, None, None, None]
    placed = rank[..., None] == jnp.arange(cap, dtype=jnp.int32)
    return (matched[..., None] & placed[None]).astype(f32)


def chosen_slots(experts, cap):
    return jnp.sum(slot_hits(experts, cap), axis=3)


def resident(value):
    return pltpu.with_memory_space_constraint(value, pltpu.VMEM)


def recurrence_kernel(
    width, got_ref, state_ref, floor_ref, gain_ref, out_ref, forget_ref, input_ref, held, sem
):
    copy = pltpu.make_async_copy(state_ref, held, sem)
    copy.start()
    lanes = got_ref.shape[2]
    heads, seq = forget_ref.shape[:2]
    half = got_ref.shape[0] // heads
    col = lanes // half
    row = lax.broadcasted_iota(jnp.int32, (2 * seq, lanes), 0)
    lane = lax.broadcasted_iota(jnp.int32, (2 * seq, lanes), 1) // col
    first, early = row < seq, row % seq < seq // 2

    def source(n):
        block = got_ref[n]
        block = block + pltpu.roll(block, 4, 0)
        block = block + pltpu.roll(block, 2, 0)
        return jnp.where(early, block, pltpu.roll(block, lanes // 2, 1))

    summed = [
        [jnp.where(first, source(2 * low * half + n), source((2 * low + 1) * half + n)) for n in range(half)]
        for low in range(heads // 2)
    ]
    scale = lax.rsqrt(summed[0][0][:, 3 * col : 3 * col + 1] / width + EPS)

    def columns(low, which):
        total = jnp.zeros((2 * seq, lanes), f32)
        for n in range(half):
            moved = pltpu.roll(summed[low][n], ((n - which) * col) % lanes, 1)
            total = jnp.where(lane == n, moved, total)
        return total * scale

    rows = []
    for low in range(heads // 2):
        query, gate, value = (columns(low, which) for which in range(3))
        floor = jnp.where(first, floor_ref[2 * low][None, :], floor_ref[2 * low + 1][None, :])
        forget = floor + (1.0 - floor) / (1.0 + jnp.exp(-gate))
        query = query / (1.0 + jnp.exp(-query))
        for k in range(2):
            forget_ref[2 * low + k] = forget[k * seq : (k + 1) * seq]
            input_ref[2 * low + k] = value[k * seq : (k + 1) * seq]
        fresh = jnp.sum(query * (1.0 - forget), axis=1, keepdims=True)
        rows.append((fresh * value, (query * forget).T))
    copy.wait()
    gain = gain_ref[...].astype(f32)
    for low in range(heads // 2):
        fresh, kept = rows[low]
        old = []
        for k in range(2):
            for t in range(seq):
                r = k * seq + t
                old.append(
                    jnp.sum(kept[:, r : r + 1] * held[t, 2 * low + k], axis=0, keepdims=True)
                )
        reads = fresh + jnp.concatenate(old, axis=0)
        mean_sq = jnp.mean(reads * reads, axis=1, keepdims=True)
        normed = (reads * lax.rsqrt(mean_sq + EPS) * gain).astype(bf16)
        for k in range(2):
            head = 2 * low + k
            block = normed[k * seq : (k + 1) * seq]
            for n in range(out_ref.shape[0]):
                out_ref[n, :, head * lanes : (head + 1) * lanes] = block


def recurrence(width, sources, got, state, floors, gain):
    seq, heads, lanes = state.shape[:3]
    return pl.pallas_call(
        lambda *refs: recurrence_kernel(width, *refs),
        out_shape=(
            jax.ShapeDtypeStruct((sources, seq, heads * lanes), bf16),
            jax.ShapeDtypeStruct((heads, seq, lanes), f32),
            jax.ShapeDtypeStruct((heads, seq, lanes), f32),
        ),
        in_specs=[
            pl.BlockSpec(memory_space=pltpu.VMEM),
            pl.BlockSpec(memory_space=pl.ANY),
            pl.BlockSpec(memory_space=pltpu.VMEM),
            pl.BlockSpec(memory_space=pltpu.VMEM),
        ],
        out_specs=tuple(pl.BlockSpec(memory_space=pltpu.VMEM) for _ in range(3)),
        scratch_shapes=[pltpu.VMEM(state.shape, f32), pltpu.SemaphoreType.DMA],
        name="recurrence",
    )(resident(got), state, floors, gain)


def experts_kernel(
    rows_v, gain_ref, gu0_ref, down0_ref, gu1_ref, down1_ref, rider_ref, out_ref,
    second, gu_v, down_v, out_v, sems, out_sems,
):
    copies = [
        pltpu.make_async_copy(src, dst, sems.at[n])
        for n, (src, dst) in enumerate(
            (
                (gu0_ref, gu_v.at[0]),
                (gu1_ref, gu_v.at[1]),
                (down0_ref, down_v.at[0]),
                (down1_ref, down_v.at[1]),
            )
        )
    ]
    for copy in copies:
        copy.start()
    sources, parts, height, lanes = rows_v.shape
    count = parts * height
    zh, feat = out_v.shape[2], out_v.shape[3] - lanes
    out_v[:, :, :, feat:] = rider_ref[...]
    total = jnp.zeros((count, lanes), f32)
    for n in range(sources):
        block = rows_v[n].reshape(count, lanes).astype(f32)
        total = total + block * block
    scale = lax.rsqrt(jnp.sum(total, axis=1, keepdims=True) / (sources * lanes) + EPS)
    for n in range(sources):
        block = rows_v[n].reshape(count, lanes).astype(f32)
        second[:, n * lanes : (n + 1) * lanes] = (block * scale * gain_ref[n]).astype(bf16)
    copies[0].wait()
    copies[1].wait()
    hidden = []
    for k in range(2):
        both = jnp.dot(second[...], gu_v[k], preferred_element_type=f32)
        gate = both[:, :lanes]
        hidden.append((gate / (1.0 + jnp.exp(-gate)) * both[:, lanes:]).astype(bf16))
    copies[2].wait()
    copies[3].wait()
    outs = []
    for part in range(parts):
        at = slice(part * feat, (part + 1) * feat)
        piece = jnp.dot(hidden[0], down_v[0, :, at], preferred_element_type=f32)
        piece = piece + jnp.dot(hidden[1], down_v[1, :, at], preferred_element_type=f32)
        out_v[:, part, :, :feat] = piece.astype(bf16).reshape(count // zh, zh, feat)
        outs.append(pltpu.make_async_copy(out_v.at[:, part], out_ref.at[:, part], out_sems.at[part]))
        outs[-1].start()
    for copy in outs:
        copy.wait()


def experts(block, gain, weights_of, rider):
    sources, parts, height, lanes = block.shape
    (gate_up, down), (gate_up_1, down_1) = weights_of
    zh = rider.shape[2]
    feat = gate_up.shape[0] // parts
    count = parts * height
    whole = (count // zh, parts, zh, feat + lanes)
    anywhere = pl.BlockSpec(memory_space=pl.ANY)
    vmem = pl.BlockSpec(memory_space=pltpu.VMEM)
    return pl.pallas_call(
        experts_kernel,
        out_shape=jax.ShapeDtypeStruct(whole, bf16),
        in_specs=[vmem, vmem, anywhere, anywhere, anywhere, anywhere, vmem],
        out_specs=anywhere,
        scratch_shapes=[
            pltpu.VMEM((count, gate_up.shape[0]), bf16),
            pltpu.VMEM((2, *gate_up.shape), bf16),
            pltpu.VMEM((2, *down.shape), bf16),
            pltpu.VMEM(whole, bf16),
            pltpu.SemaphoreType.DMA((4,)),
            pltpu.SemaphoreType.DMA((parts,)),
        ],
        name="experts",
    )(resident(block), gain, gate_up, down, gate_up_1, down_1, rider)


def shards(
    tokens,
    norm_gain,
    w_query,
    w_forget,
    w_input,
    forget_floor,
    head_gain,
    w_output,
    state,
    ffn_gain,
    route_experts,
    route_weights,
    w_gate,
    w_up,
    w_down,
):
    tp = lax.axis_size("tp")
    rows = lax.axis_size(ROW)
    zh = lax.axis_size(ZH)
    seq, feat = tokens.shape
    width = feat * tp
    heads, head = state.shape[1], state.shape[2]
    col = w_query.shape[1]
    low = zh // tp
    here = lax.axis_index(ROW)
    c = lax.axis_size("c")
    chips = rows // c
    cap = max(2, seq // 2)

    routes = jnp.pad(route_experts.astype(bf16), ((0, 0), (0, feat - route_experts.shape[1])))
    all_rows = jnp.concatenate([tokens, routes], axis=0)
    for axis in GATHER[:2]:
        all_rows = lax.all_gather(all_rows, axis, tiled=True)

    w_joint = jnp.concatenate([w_query, w_forget, w_input, w_output], axis=1).T
    w_joint, all_rows = lax.optimization_barrier((w_joint, all_rows))
    w_all = gathered(w_joint, "za", tp)
    for axis in GATHER[2:]:
        all_rows = lax.all_gather(all_rows, axis, tiled=True)
    all_rows = all_rows.reshape(2, 2, 2, 2, 2, 2, seq, feat)
    order = tuple(GATHER[::-1].index(axis) for axis in WIDE)
    all_rows = all_rows.transpose(*order, 5, 6, 7).reshape(2 * rows, 2, seq, feat)
    mine = lax.dynamic_slice_in_dim(all_rows, lax.axis_index("zm") * rows, rows, 0)
    experts_all = mine[:, 1, :, : route_experts.shape[1]].astype(jnp.int32)
    tok_mine = mine[:, 0].reshape(rows * seq, feat)
    w_all, tok_all = lax.optimization_barrier(
        (w_all, all_rows[:, 0].reshape(2 * rows * seq, feat))
    )

    tok_all = tok_all.astype(f32)
    sum_sq = jnp.sum(tok_all * tok_all, axis=1)
    scaled = (tok_all * norm_gain.astype(f32)).astype(bf16)
    partial = jnp.einsum("td,pcd->tpc", scaled, w_all[:, : 3 * col], preferred_element_type=f32)
    partial = partial.reshape(2 * rows, seq, tp, 3 * col).transpose(0, 2, 1, 3)
    share = feat // (2 * rows * seq)
    rest = LANES // 2 - 3 * col - share
    gain_here = lax.dynamic_index_in_dim(
        ffn_gain.astype(f32).reshape(2 * rows, seq, share), lax.axis_index(WIDE), 0, False
    )
    gain_sent = jnp.broadcast_to(gain_here, (2 * rows, tp, seq, share))
    stat = jnp.broadcast_to(sum_sq.reshape(2 * rows, 1, seq, 1), (2 * rows, tp, seq, rest))
    sent = jnp.concatenate([partial, stat, gain_sent], axis=3)
    sent = sent.reshape(2 * rows * tp, 2, seq // 2, LANES // 2).transpose(0, 2, 1, 3)
    got = exchange(sent.reshape(2 * rows * tp, seq // 2, LANES), (*WIDE, "tp"))
    got = got.reshape(2 * rows, tp * seq // 2, LANES)

    w_out = lax.all_gather(w_all[:, 3 * col :], "zm", axis=1).reshape(tp, low * col, feat)
    got, w_out = lax.optimization_barrier((got, w_out))

    heads_sent, forget, inputs = recurrence(
        width, rows, got, state, forget_floor.reshape(heads, head), head_gain.reshape(1, head)
    )
    forget, inputs = forget.transpose(1, 0, 2), inputs.transpose(1, 0, 2)
    new_state = forget[..., None] * state + (1.0 - forget)[..., None] * inputs[:, :, None, :]

    quarter = rows // tp
    sel = chosen_slots(experts_all, cap).reshape(EXPERTS, tp, quarter, seq, cap)
    sel = sel.transpose(0, 1, 4, 2, 3)
    eye = jnp.eye(rows, dtype=f32).reshape(tp, quarter, rows)
    sel = sel[:, :, :, :, None, :] * eye[None, :, None, :, :, None]
    sel = sel.reshape(EXPERTS * rows * cap, rows * seq).astype(bf16)

    heads_all = exchange(heads_sent, ROW).reshape(rows * seq, feat)
    part_out = jnp.einsum("td,pcd->tpc", heads_all, w_out, preferred_element_type=f32)
    residual = lax.dynamic_index_in_dim(
        tok_mine.astype(f32).reshape(rows * seq, low, rows, col), here, 2, False
    ).reshape(rows * seq, 1, low * col)
    own = (jnp.arange(tp) == lax.axis_index("tp"))[None, :, None]
    with_tok = (part_out + jnp.where(own, residual, 0.0)).reshape(rows * seq, tp * low * col)

    outgoing = jnp.dot(sel, with_tok.astype(bf16), preferred_element_type=f32).astype(bf16)
    arrived = exchange(outgoing.reshape(zh * tp, cap * quarter, LANES), (*ZH, "tp"))
    arrived = arrived.astype(f32).reshape(zh, tp, cap, quarter, LANES).sum(axis=1).astype(bf16)
    arrived = arrived.transpose(1, 2, 0, 3).reshape(cap, quarter * zh, LANES)
    sent = jnp.broadcast_to(
        arrived[None, :, None], (chips, c, tp, quarter * zh, LANES)
    ).reshape(rows * tp, quarter * zh, LANES)
    block = exchange(sent, PAIR).reshape(rows, tp, quarter * zh, LANES)

    def ordered(w):
        return w.reshape(zh, rows, col, -1).transpose(1, 0, 2, 3).reshape(width, -1)

    units = w_gate.shape[2]
    fill = ((0, 0), (0, LANES - units))
    gate_up = jnp.concatenate(
        [jnp.pad(ordered(w_gate[0]), fill), jnp.pad(ordered(w_up[0]), fill)], axis=1
    )
    down = jnp.pad(w_down[0], fill[::-1])
    weights_of = [(gate_up, down), tuple(lax.ppermute(w, "c", [(0, 1), (1, 0)]) for w in (gate_up, down))]

    gain_all = got.reshape(2 * rows, tp, seq // 2, 2, LANES // 2)[..., LANES // 2 - share :]
    gain_all = gain_all.transpose(1, 0, 3, 2, 4)
    gain_all = ordered(gain_all.reshape(width, 1)).reshape(rows, 1, LANES)
    rider = part_out.reshape(rows, seq, tp, low * col).transpose(0, 2, 1, 3)
    rider = jnp.pad(rider.astype(bf16), ((0, 0), (0, 0), (0, zh - seq), (0, LANES - low * col)))
    back = experts(block, gain_all, weights_of, rider)
    back = back.reshape(rows * tp, zh, feat + LANES)
    back = exchange(back, PAIR).astype(f32)
    summed = back[:, :, :feat].reshape(chips, c, tp, zh, feat).sum(axis=(0, 2)).astype(bf16)
    returned = exchange(summed.transpose(1, 0, 2), ZH).astype(f32)
    mixer = back[:, :seq, feat : feat + low * col].reshape(rows, tp, seq, low, col).sum(axis=1)
    mixer = mixer.transpose(1, 2, 0, 3).reshape(seq, feat).astype(bf16)
    middle = (tokens.astype(f32) + mixer.astype(f32)).astype(bf16)

    hits = slot_hits(route_experts[None], cap)[:, 0]
    weights = jnp.sum(hits * route_weights[None, :, :, None], axis=2)
    routed = jnp.einsum("ets,esd->td", weights, returned, precision=lax.Precision.HIGHEST)
    mixed = (middle.astype(f32) + routed).astype(bf16)
    return mixed, new_state


def solution(mesh):
    torus = Mesh(mesh.devices.reshape(4, 2, 2, 2, 2, 2, mesh.shape["tp"]), (*EP, "tp"))
    in_specs = (
        P(EP, "tp"),
        P("tp"),
        P("tp", EP),
        P("tp", EP),
        P("tp", EP),
        P("tp"),
        P(),
        P("tp", EP),
        P(EP, "tp", None, None),
        P("tp"),
        P(EP, None),
        P(EP, None),
        P(EP, None, "tp"),
        P(EP, None, "tp"),
        P(EP, "tp", None),
    )
    out_specs = (P(EP, "tp"), P(EP, "tp", None, None))
    return jax.shard_map(
        shards, mesh=torus, in_specs=in_specs, out_specs=out_specs, check_vma=False
    )
```

```python
import jax
import jax.numpy as jnp
from jax import lax
from jax.experimental import pallas as pl
from jax.experimental.pallas import tpu as pltpu
from jax.sharding import Mesh
from jax.sharding import PartitionSpec as P

EXPERTS = 8
EPS = 1e-06
LANES = 128
EP = ("zh", "zl", "xh", "xl", "c")
ROW = ("zl", "xh", "xl", "c")
PAIR = (*ROW, "tp")
GATHER = ("c", "xl", "xh", "zl")
bf16 = jnp.bfloat16
f32 = jnp.float32


def exchange(blocks, axes):
    return lax.all_to_all(blocks, axes, split_axis=0, concat_axis=0, tiled=True)


def gathered(shard, axes, count):
    return exchange(jnp.broadcast_to(shard[None], (count, *shard.shape)), axes)


def slot_hits(experts, cap):
    positions = jnp.arange(experts.shape[1], dtype=jnp.int32)
    earlier = positions[None, :] < positions[:, None]
    same = experts[:, :, :, None, None] == experts[:, None, None, :, :]
    rank = jnp.sum(same & earlier[None, :, None, :, None], axis=(3, 4))
    matched = experts[None] == jnp.arange(EXPERTS, dtype=jnp.int32)[:, None, None, None]
    placed = rank[..., None] == jnp.arange(cap, dtype=jnp.int32)
    return (matched[..., None] & placed[None]).astype(f32)


def chosen_slots(experts, cap):
    return jnp.sum(slot_hits(experts, cap), axis=3)


def resident(value):
    return pltpu.with_memory_space_constraint(value, pltpu.VMEM)


def recurrence_kernel(
    width, got_ref, held, floor_ref, gain_ref, out_ref, forget_ref, input_ref
):
    sources, parts, seq, lanes = got_ref.shape
    heads = forget_ref.shape[0]
    half = sources // 2
    col = lanes // half
    summed = []
    for s in range(half):
        both = []
        for source in (s, s + half):
            block = got_ref[source, 0]
            for part in range(1, parts):
                block = block + got_ref[source, part]
            both.append(block)
        summed.append(jnp.concatenate(both, axis=0))
    stat = summed[0][:seq, lanes - 1 :]
    scale = lax.rsqrt(stat / width + EPS)
    scale = jnp.concatenate([scale, scale], axis=0)
    lane = lax.broadcasted_iota(jnp.int32, (2 * seq, lanes), 1) // col
    first = lax.broadcasted_iota(jnp.int32, (2 * seq, lanes), 0) < seq

    def columns(low, which):
        total = jnp.zeros((2 * seq, lanes), f32)
        at = (low * 3 + which) * col
        for s in range(half):
            moved = pltpu.roll(summed[s], (s * col - at) % lanes, 1)
            total = jnp.where(lane == s, moved, total)
        return total * scale

    rows = []
    for low in range(heads // 2):
        query, gate, value = (columns(low, which) for which in range(3))
        floor = jnp.where(first, floor_ref[2 * low][None, :], floor_ref[2 * low + 1][None, :])
        forget = floor + (1.0 - floor) / (1.0 + jnp.exp(-gate))
        query = query / (1.0 + jnp.exp(-query))
        for k in range(2):
            forget_ref[2 * low + k] = forget[k * seq : (k + 1) * seq]
            input_ref[2 * low + k] = value[k * seq : (k + 1) * seq]
        fresh = jnp.sum(query * (1.0 - forget), axis=1, keepdims=True)
        rows.append((fresh * value, (query * forget).T))
    gain = gain_ref[...].astype(f32)
    for low in range(heads // 2):
        fresh, kept = rows[low]
        old = []
        for k in range(2):
            for t in range(seq):
                r = k * seq + t
                old.append(
                    jnp.sum(kept[:, r : r + 1] * held[t, 2 * low + k], axis=0, keepdims=True)
                )
        reads = fresh + jnp.concatenate(old, axis=0)
        mean_sq = jnp.mean(reads * reads, axis=1, keepdims=True)
        normed = (reads * lax.rsqrt(mean_sq + EPS) * gain).astype(bf16)
        for k in range(2):
            head = 2 * low + k
            block = normed[k * seq : (k + 1) * seq]
            for n in range(out_ref.shape[0]):
                out_ref[n, :, head * lanes : (head + 1) * lanes] = block


def recurrence(width, got, state, floors, gain):
    sources, _, seq, lanes = got.shape
    heads = state.shape[1]
    return pl.pallas_call(
        lambda *refs: recurrence_kernel(width, *refs),
        out_shape=(
            jax.ShapeDtypeStruct((sources, seq, heads * lanes), bf16),
            jax.ShapeDtypeStruct((heads, seq, lanes), f32),
            jax.ShapeDtypeStruct((heads, seq, lanes), f32),
        ),
        in_specs=[
            pl.BlockSpec(memory_space=pltpu.VMEM),
            pl.BlockSpec(memory_space=pltpu.VMEM),
            pl.BlockSpec(memory_space=pltpu.VMEM),
            pl.BlockSpec(memory_space=pltpu.VMEM),
        ],
        out_specs=tuple(pl.BlockSpec(memory_space=pltpu.VMEM) for _ in range(3)),
        name="recurrence",
    )(resident(got), resident(state), floors, gain)


def experts_kernel(
    rows_v, gain_ref, gu0_ref, down0_ref, gu1_ref, down1_ref, rider_ref, out_ref,
    second, gu_v, down_v, out_v, sems, out_sems,
):
    copies = [
        pltpu.make_async_copy(src, dst, sems.at[n])
        for n, (src, dst) in enumerate(
            (
                (gu0_ref, gu_v.at[0]),
                (gu1_ref, gu_v.at[1]),
                (down0_ref, down_v.at[0]),
                (down1_ref, down_v.at[1]),
            )
        )
    ]
    for copy in copies:
        copy.start()
    sources, parts, height, lanes = rows_v.shape
    count = parts * height
    zh, feat = out_v.shape[2], out_v.shape[3] - lanes
    out_v[:, :, :, feat:] = rider_ref[...]
    total = jnp.zeros((count, lanes), f32)
    for n in range(sources):
        block = rows_v[n].reshape(count, lanes).astype(f32)
        total = total + block * block
    scale = lax.rsqrt(jnp.sum(total, axis=1, keepdims=True) / (sources * lanes) + EPS)
    for n in range(sources):
        block = rows_v[n].reshape(count, lanes).astype(f32)
        second[:, n * lanes : (n + 1) * lanes] = (block * scale * gain_ref[n]).astype(bf16)
    copies[0].wait()
    copies[1].wait()
    hidden = []
    for k in range(2):
        both = jnp.dot(second[...], gu_v[k], preferred_element_type=f32)
        gate = both[:, :lanes]
        hidden.append((gate / (1.0 + jnp.exp(-gate)) * both[:, lanes:]).astype(bf16))
    copies[2].wait()
    copies[3].wait()
    outs = []
    for part in range(parts):
        at = slice(part * feat, (part + 1) * feat)
        piece = jnp.dot(hidden[0], down_v[0, :, at], preferred_element_type=f32)
        piece = piece + jnp.dot(hidden[1], down_v[1, :, at], preferred_element_type=f32)
        out_v[:, part, :, :feat] = piece.astype(bf16).reshape(count // zh, zh, feat)
        outs.append(pltpu.make_async_copy(out_v.at[:, part], out_ref.at[:, part], out_sems.at[part]))
        outs[-1].start()
    for copy in outs:
        copy.wait()


def experts(block, gain, weights_of, rider):
    sources, parts, height, lanes = block.shape
    (gate_up, down), (gate_up_1, down_1) = weights_of
    zh = rider.shape[2]
    feat = gate_up.shape[0] // parts
    count = parts * height
    whole = (count // zh, parts, zh, feat + lanes)
    anywhere = pl.BlockSpec(memory_space=pl.ANY)
    vmem = pl.BlockSpec(memory_space=pltpu.VMEM)
    return pl.pallas_call(
        experts_kernel,
        out_shape=jax.ShapeDtypeStruct(whole, bf16),
        in_specs=[vmem, vmem, anywhere, anywhere, anywhere, anywhere, vmem],
        out_specs=anywhere,
        scratch_shapes=[
            pltpu.VMEM((count, gate_up.shape[0]), bf16),
            pltpu.VMEM((2, *gate_up.shape), bf16),
            pltpu.VMEM((2, *down.shape), bf16),
            pltpu.VMEM(whole, bf16),
            pltpu.SemaphoreType.DMA((4,)),
            pltpu.SemaphoreType.DMA((parts,)),
        ],
        name="experts",
    )(resident(block), gain, gate_up, down, gate_up_1, down_1, rider)


def shards(
    tokens,
    norm_gain,
    w_query,
    w_forget,
    w_input,
    forget_floor,
    head_gain,
    w_output,
    state,
    ffn_gain,
    route_experts,
    route_weights,
    w_gate,
    w_up,
    w_down,
):
    tp = lax.axis_size("tp")
    rows = lax.axis_size(ROW)
    zh = lax.axis_size("zh")
    seq, feat = tokens.shape
    width = feat * tp
    heads, head = state.shape[1], state.shape[2]
    col = w_query.shape[1]
    low = zh // tp
    here = lax.axis_index(ROW)
    c = lax.axis_size("c")
    chips = rows // c
    cap = max(2, seq // 2)

    w_joint = jnp.concatenate([w_query, w_forget, w_input, w_output], axis=1).T
    w_all = gathered(w_joint, "zh", zh)

    routes = jnp.pad(route_experts.astype(bf16), ((0, 0), (0, feat - route_experts.shape[1])))
    all_rows = jnp.concatenate([tokens, routes], axis=0)
    for axis in GATHER:
        all_rows = lax.all_gather(all_rows, axis, tiled=True)

    all_rows = all_rows.reshape(2, 2, 2, 2, 2, seq, feat)
    order = tuple(GATHER[::-1].index(axis) for axis in ROW)
    all_rows = all_rows.transpose(*order, 4, 5, 6).reshape(rows, 2, seq, feat)
    experts_all = all_rows[:, 1, :, : route_experts.shape[1]].astype(jnp.int32)
    w_all, tok_all = lax.optimization_barrier((w_all, all_rows[:, 0].reshape(rows * seq, feat)))
    w_in = w_all[:, : 3 * col].reshape(tp, low * 3 * col, feat)
    w_out = w_all[:, 3 * col :].reshape(tp, low * col, feat)

    tok_all = tok_all.astype(f32)
    sum_sq = jnp.sum(tok_all * tok_all, axis=1)
    scaled = (tok_all * norm_gain.astype(f32)).astype(bf16)
    partial = jnp.einsum("td,pcd->tpc", scaled, w_in, preferred_element_type=f32)
    partial = partial.reshape(rows, seq, tp, low * 3 * col).transpose(0, 2, 1, 3)
    used = low * 3 * col
    share = feat // (rows * seq)
    gain_here = lax.dynamic_index_in_dim(
        ffn_gain.astype(f32).reshape(rows, seq, share), here, 0, False
    )
    gain_sent = jnp.broadcast_to(gain_here, (rows, tp, seq, share))
    stat = jnp.broadcast_to(sum_sq.reshape(rows, 1, seq, 1), (rows, tp, seq, LANES - used - share))
    sent = jnp.concatenate([partial, gain_sent, stat], axis=3).reshape(rows * tp, seq, LANES)
    got = exchange(sent, PAIR).reshape(rows, tp, seq, LANES)

    heads_sent, forget, inputs = recurrence(
        width, got, state, forget_floor.reshape(heads, head), head_gain.reshape(1, head)
    )
    forget, inputs = forget.transpose(1, 0, 2), inputs.transpose(1, 0, 2)
    new_state = forget[..., None] * state + (1.0 - forget)[..., None] * inputs[:, :, None, :]

    quarter = rows // tp
    sel = chosen_slots(experts_all, cap).reshape(EXPERTS, tp, quarter, seq, cap)
    sel = sel.transpose(0, 1, 4, 2, 3)
    eye = jnp.eye(rows, dtype=f32).reshape(tp, quarter, rows)
    sel = sel[:, :, :, :, None, :] * eye[None, :, None, :, :, None]
    sel = sel.reshape(EXPERTS * rows * cap, rows * seq).astype(bf16)

    heads_all = exchange(heads_sent, ROW).reshape(rows * seq, feat)
    part_out = jnp.einsum("td,pcd->tpc", heads_all, w_out, preferred_element_type=f32)
    residual = lax.dynamic_index_in_dim(
        tok_all.reshape(rows * seq, low, rows, col), here, 2, False
    ).reshape(rows * seq, 1, low * col)
    own = (jnp.arange(tp) == lax.axis_index("tp"))[None, :, None]
    with_tok = (part_out + jnp.where(own, residual, 0.0)).reshape(rows * seq, tp * low * col)

    outgoing = jnp.dot(sel, with_tok.astype(bf16), preferred_element_type=f32).astype(bf16)
    arrived = exchange(outgoing.reshape(zh * tp, cap * quarter, LANES), ("zh", "tp"))
    arrived = arrived.astype(f32).reshape(zh, tp, cap, quarter, LANES).sum(axis=1).astype(bf16)
    arrived = arrived.transpose(1, 2, 0, 3).reshape(cap, quarter * zh, LANES)
    sent = jnp.broadcast_to(
        arrived[None, :, None], (chips, c, tp, quarter * zh, LANES)
    ).reshape(rows * tp, quarter * zh, LANES)
    block = exchange(sent, PAIR).reshape(rows, tp, quarter * zh, LANES)

    def ordered(w):
        return w.reshape(zh, rows, col, -1).transpose(1, 0, 2, 3).reshape(width, -1)

    units = w_gate.shape[2]
    fill = ((0, 0), (0, LANES - units))
    gate_up = jnp.concatenate(
        [jnp.pad(ordered(w_gate[0]), fill), jnp.pad(ordered(w_up[0]), fill)], axis=1
    )
    down = jnp.pad(w_down[0], fill[::-1])
    weights_of = [(gate_up, down), tuple(lax.ppermute(w, "c", [(0, 1), (1, 0)]) for w in (gate_up, down))]

    gain_all = got[:, :, :, used : used + share].transpose(1, 0, 2, 3)
    gain_all = ordered(gain_all.reshape(width, 1)).reshape(rows, 1, LANES)
    rider = part_out.reshape(rows, seq, tp, low * col).transpose(0, 2, 1, 3)
    rider = jnp.pad(rider.astype(bf16), ((0, 0), (0, 0), (0, zh - seq), (0, LANES - low * col)))
    back = experts(block, gain_all, weights_of, rider)
    back = back.reshape(rows * tp, zh, feat + LANES)
    back = exchange(back, PAIR).astype(f32)
    summed = back[:, :, :feat].reshape(chips, c, tp, zh, feat).sum(axis=(0, 2)).astype(bf16)
    returned = exchange(summed.transpose(1, 0, 2), "zh").astype(f32)
    mixer = back[:, :seq, feat : feat + low * col].reshape(rows, tp, seq, low, col).sum(axis=1)
    mixer = mixer.transpose(1, 2, 0, 3).reshape(seq, feat).astype(bf16)
    middle = (tokens.astype(f32) + mixer.astype(f32)).astype(bf16)

    hits = slot_hits(route_experts[None], cap)[:, 0]
    weights = jnp.sum(hits * route_weights[None, :, :, None], axis=2)
    routed = jnp.einsum("ets,esd->td", weights, returned, precision=lax.Precision.HIGHEST)
    mixed = (middle.astype(f32) + routed).astype(bf16)
    return mixed, new_state


def solution(mesh):
    torus = Mesh(mesh.devices.reshape(8, 2, 2, 2, 2, mesh.shape["tp"]), (*EP, "tp"))
    in_specs = (
        P(EP, "tp"),
        P("tp"),
        P("tp", EP),
        P("tp", EP),
        P("tp", EP),
        P("tp"),
        P(),
        P("tp", EP),
        P(EP, "tp", None, None),
        P("tp"),
        P(EP, None),
        P(EP, None),
        P(EP, None, "tp"),
        P(EP, None, "tp"),
        P(EP, "tp", None),
    )
    out_specs = (P(EP, "tp"), P(EP, "tp", None, None))
    return jax.shard_map(
        shards, mesh=torus, in_specs=in_specs, out_specs=out_specs, check_vma=False
    )
```

```python
import jax
import jax.numpy as jnp
from jax import lax
from jax.experimental import pallas as pl
from jax.experimental.pallas import tpu as pltpu
from jax.sharding import Mesh
from jax.sharding import PartitionSpec as P

EXPERTS = 8
EPS = 1e-06
LANES = 128
ZH = ("za", "zm")
EP = (*ZH, "zl", "xh", "xl", "c")
ROW = ("zl", "xh", "xl", "c")
PAIR = (*ROW, "tp")
GATHER = ("c", "xl", "xh", "zl")
bf16 = jnp.bfloat16
f32 = jnp.float32


def exchange(blocks, axes):
    return lax.all_to_all(blocks, axes, split_axis=0, concat_axis=0, tiled=True)


def gathered(shard, axes, count):
    return exchange(jnp.broadcast_to(shard[None], (count, *shard.shape)), axes)


def slot_hits(experts, cap):
    positions = jnp.arange(experts.shape[1], dtype=jnp.int32)
    earlier = positions[None, :] < positions[:, None]
    same = experts[:, :, :, None, None] == experts[:, None, None, :, :]
    rank = jnp.sum(same & earlier[None, :, None, :, None], axis=(3, 4))
    matched = experts[None] == jnp.arange(EXPERTS, dtype=jnp.int32)[:, None, None, None]
    placed = rank[..., None] == jnp.arange(cap, dtype=jnp.int32)
    return (matched[..., None] & placed[None]).astype(f32)


def chosen_slots(experts, cap):
    return jnp.sum(slot_hits(experts, cap), axis=3)


def resident(value):
    return pltpu.with_memory_space_constraint(value, pltpu.VMEM)


def recurrence_kernel(
    width, got_ref, held, floor_ref, gain_ref, out_ref, forget_ref, input_ref
):
    sources, parts, seq, lanes = got_ref.shape
    heads = forget_ref.shape[0]
    half = sources // 2
    col = lanes // half
    summed = []
    for s in range(half):
        both = []
        for source in (s, s + half):
            block = got_ref[source, 0]
            for part in range(1, parts):
                block = block + got_ref[source, part]
            both.append(block)
        summed.append(jnp.concatenate(both, axis=0))
    stat = summed[0][:seq, lanes - 1 :]
    scale = lax.rsqrt(stat / width + EPS)
    scale = jnp.concatenate([scale, scale], axis=0)
    lane = lax.broadcasted_iota(jnp.int32, (2 * seq, lanes), 1) // col
    first = lax.broadcasted_iota(jnp.int32, (2 * seq, lanes), 0) < seq

    def columns(low, which):
        total = jnp.zeros((2 * seq, lanes), f32)
        at = (low * 3 + which) * col
        for s in range(half):
            moved = pltpu.roll(summed[s], (s * col - at) % lanes, 1)
            total = jnp.where(lane == s, moved, total)
        return total * scale

    rows = []
    for low in range(heads // 2):
        query, gate, value = (columns(low, which) for which in range(3))
        floor = jnp.where(first, floor_ref[2 * low][None, :], floor_ref[2 * low + 1][None, :])
        forget = floor + (1.0 - floor) / (1.0 + jnp.exp(-gate))
        query = query / (1.0 + jnp.exp(-query))
        for k in range(2):
            forget_ref[2 * low + k] = forget[k * seq : (k + 1) * seq]
            input_ref[2 * low + k] = value[k * seq : (k + 1) * seq]
        fresh = jnp.sum(query * (1.0 - forget), axis=1, keepdims=True)
        rows.append((fresh * value, (query * forget).T))
    gain = gain_ref[...].astype(f32)
    for low in range(heads // 2):
        fresh, kept = rows[low]
        old = []
        for k in range(2):
            for t in range(seq):
                r = k * seq + t
                old.append(
                    jnp.sum(kept[:, r : r + 1] * held[t, 2 * low + k], axis=0, keepdims=True)
                )
        reads = fresh + jnp.concatenate(old, axis=0)
        mean_sq = jnp.mean(reads * reads, axis=1, keepdims=True)
        normed = (reads * lax.rsqrt(mean_sq + EPS) * gain).astype(bf16)
        for k in range(2):
            head = 2 * low + k
            block = normed[k * seq : (k + 1) * seq]
            for n in range(out_ref.shape[0]):
                out_ref[n, :, head * lanes : (head + 1) * lanes] = block


def recurrence(width, got, state, floors, gain):
    sources, _, seq, lanes = got.shape
    heads = state.shape[1]
    return pl.pallas_call(
        lambda *refs: recurrence_kernel(width, *refs),
        out_shape=(
            jax.ShapeDtypeStruct((sources, seq, heads * lanes), bf16),
            jax.ShapeDtypeStruct((heads, seq, lanes), f32),
            jax.ShapeDtypeStruct((heads, seq, lanes), f32),
        ),
        in_specs=[
            pl.BlockSpec(memory_space=pltpu.VMEM),
            pl.BlockSpec(memory_space=pltpu.VMEM),
            pl.BlockSpec(memory_space=pltpu.VMEM),
            pl.BlockSpec(memory_space=pltpu.VMEM),
        ],
        out_specs=tuple(pl.BlockSpec(memory_space=pltpu.VMEM) for _ in range(3)),
        name="recurrence",
    )(resident(got), resident(state), floors, gain)


def experts_kernel(
    rows_v, gain_ref, gu0_ref, down0_ref, gu1_ref, down1_ref, rider_ref, out_ref,
    second, gu_v, down_v, out_v, sems, out_sems,
):
    copies = [
        pltpu.make_async_copy(src, dst, sems.at[n])
        for n, (src, dst) in enumerate(
            (
                (gu0_ref, gu_v.at[0]),
                (gu1_ref, gu_v.at[1]),
                (down0_ref, down_v.at[0]),
                (down1_ref, down_v.at[1]),
            )
        )
    ]
    for copy in copies:
        copy.start()
    sources, parts, height, lanes = rows_v.shape
    count = parts * height
    zh, feat = out_v.shape[2], out_v.shape[3] - lanes
    out_v[:, :, :, feat:] = rider_ref[...]
    total = jnp.zeros((count, lanes), f32)
    for n in range(sources):
        block = rows_v[n].reshape(count, lanes).astype(f32)
        total = total + block * block
    scale = lax.rsqrt(jnp.sum(total, axis=1, keepdims=True) / (sources * lanes) + EPS)
    for n in range(sources):
        block = rows_v[n].reshape(count, lanes).astype(f32)
        second[:, n * lanes : (n + 1) * lanes] = (block * scale * gain_ref[n]).astype(bf16)
    hidden = []
    for k in range(2):
        copies[k].wait()
        both = jnp.dot(second[...], gu_v[k], preferred_element_type=f32)
        gate = both[:, :lanes]
        hidden.append((gate / (1.0 + jnp.exp(-gate)) * both[:, lanes:]).astype(bf16))
    copies[2].wait()
    copies[3].wait()
    outs = []
    for part in range(parts):
        at = slice(part * feat, (part + 1) * feat)
        piece = jnp.dot(hidden[0], down_v[0, :, at], preferred_element_type=f32)
        piece = piece + jnp.dot(hidden[1], down_v[1, :, at], preferred_element_type=f32)
        out_v[:, part, :, :feat] = piece.astype(bf16).reshape(count // zh, zh, feat)
        outs.append(pltpu.make_async_copy(out_v.at[:, part], out_ref.at[:, part], out_sems.at[part]))
        outs[-1].start()
    for copy in outs:
        copy.wait()


def experts(block, gain, weights_of, rider):
    _, parts, height, lanes = block.shape
    (gate_up, down), (gate_up_1, down_1) = weights_of
    zh = rider.shape[2]
    feat = gate_up.shape[0] // parts
    count = parts * height
    whole = (count // zh, parts, zh, feat + lanes)
    anywhere = pl.BlockSpec(memory_space=pl.ANY)
    vmem = pl.BlockSpec(memory_space=pltpu.VMEM)
    return pl.pallas_call(
        experts_kernel,
        out_shape=jax.ShapeDtypeStruct(whole, bf16),
        in_specs=[vmem, vmem, anywhere, anywhere, anywhere, anywhere, vmem],
        out_specs=anywhere,
        scratch_shapes=[
            pltpu.VMEM((count, gate_up.shape[0]), bf16),
            pltpu.VMEM((2, *gate_up.shape), bf16),
            pltpu.VMEM((2, *down.shape), bf16),
            pltpu.VMEM(whole, bf16),
            pltpu.SemaphoreType.DMA((4,)),
            pltpu.SemaphoreType.DMA((parts,)),
        ],
        name="experts",
    )(resident(block), gain, gate_up, down, gate_up_1, down_1, rider)


def shards(
    tokens,
    norm_gain,
    w_query,
    w_forget,
    w_input,
    forget_floor,
    head_gain,
    w_output,
    state,
    ffn_gain,
    route_experts,
    route_weights,
    w_gate,
    w_up,
    w_down,
):
    tp = lax.axis_size("tp")
    rows = lax.axis_size(ROW)
    zh = lax.axis_size(ZH)
    seq, feat = tokens.shape
    width = feat * tp
    heads, head = state.shape[1], state.shape[2]
    col = w_query.shape[1]
    low = zh // tp
    here = lax.axis_index(ROW)
    c = lax.axis_size("c")
    chips = rows // c
    cap = max(2, seq // 2)

    w_joint = jnp.concatenate([w_query, w_forget, w_input, w_output], axis=1).T
    w_mine = gathered(w_joint, "za", zh // 2)

    routes = jnp.pad(route_experts.astype(bf16), ((0, 0), (0, feat - route_experts.shape[1])))
    all_rows = jnp.concatenate([tokens, routes], axis=0)
    for axis in GATHER[:-1]:
        all_rows = lax.all_gather(all_rows, axis, tiled=True)
    w_mine, all_rows = lax.optimization_barrier((w_mine, all_rows))

    swap = [(0, 1), (1, 0)]
    in_mine, out_mine = w_mine[:, : 3 * col], w_mine[:, 3 * col :]
    in_other = lax.ppermute(in_mine, "zm", swap)
    out_other = lax.ppermute(out_mine, "zm", swap)
    even = lax.axis_index("zm") == 0

    def projected(rows_in, own, other):
        own, other = (
            jnp.einsum("td,pcd->tpc", rows_in, w, preferred_element_type=f32) for w in (own, other)
        )
        return jnp.where(
            even, jnp.concatenate([own, other], axis=2), jnp.concatenate([other, own], axis=2)
        )

    all_rows = lax.all_gather(all_rows, GATHER[-1], tiled=True)
    all_rows = all_rows.reshape(2, 2, 2, 2, 2, seq, feat)
    order = tuple(GATHER[::-1].index(axis) for axis in ROW)
    all_rows = all_rows.transpose(*order, 4, 5, 6).reshape(rows, 2, seq, feat)
    experts_all = all_rows[:, 1, :, : route_experts.shape[1]].astype(jnp.int32)
    tok_all = all_rows[:, 0].reshape(rows * seq, feat)

    tok_all = tok_all.astype(f32)
    sum_sq = jnp.sum(tok_all * tok_all, axis=1)
    scaled = (tok_all * norm_gain.astype(f32)).astype(bf16)
    partial = projected(scaled, in_mine, in_other)
    partial = partial.reshape(rows, seq, tp, low * 3 * col).transpose(0, 2, 1, 3)
    used = low * 3 * col
    share = feat // (rows * seq)
    gain_here = lax.dynamic_index_in_dim(
        ffn_gain.astype(f32).reshape(rows, seq, share), here, 0, False
    )
    gain_sent = jnp.broadcast_to(gain_here, (rows, tp, seq, share))
    stat = jnp.broadcast_to(sum_sq.reshape(rows, 1, seq, 1), (rows, tp, seq, LANES - used - share))
    sent = jnp.concatenate([partial, gain_sent, stat], axis=3).reshape(rows * tp, seq, LANES)
    got = exchange(sent, PAIR).reshape(rows, tp, seq, LANES)

    heads_sent, forget, inputs = recurrence(
        width, got, state, forget_floor.reshape(heads, head), head_gain.reshape(1, head)
    )
    forget, inputs = forget.transpose(1, 0, 2), inputs.transpose(1, 0, 2)
    new_state = forget[..., None] * state + (1.0 - forget)[..., None] * inputs[:, :, None, :]

    quarter = rows // tp
    sel = chosen_slots(experts_all, cap).reshape(EXPERTS, tp, quarter, seq, cap)
    sel = sel.transpose(0, 1, 4, 2, 3)
    eye = jnp.eye(rows, dtype=f32).reshape(tp, quarter, rows)
    sel = sel[:, :, :, :, None, :] * eye[None, :, None, :, :, None]
    sel = sel.reshape(EXPERTS * rows * cap, rows * seq).astype(bf16)

    heads_all = exchange(heads_sent, ROW).reshape(rows * seq, feat)
    part_out = projected(heads_all, out_mine, out_other)
    residual = lax.dynamic_index_in_dim(
        tok_all.reshape(rows * seq, low, rows, col), here, 2, False
    ).reshape(rows * seq, 1, low * col)
    own = (jnp.arange(tp) == lax.axis_index("tp"))[None, :, None]
    with_tok = (part_out + jnp.where(own, residual, 0.0)).reshape(rows * seq, tp * low * col)

    outgoing = jnp.dot(sel, with_tok.astype(bf16), preferred_element_type=f32).astype(bf16)
    arrived = exchange(outgoing.reshape(zh * tp, cap * quarter, LANES), (*ZH, "tp"))
    arrived = arrived.astype(f32).reshape(zh, tp, cap, quarter, LANES).sum(axis=1).astype(bf16)
    arrived = arrived.transpose(1, 2, 0, 3).reshape(cap, quarter * zh, LANES)
    sent = jnp.broadcast_to(
        arrived[None, :, None], (chips, c, tp, quarter * zh, LANES)
    ).reshape(rows * tp, quarter * zh, LANES)
    block = exchange(sent, PAIR).reshape(rows, tp, quarter * zh, LANES)

    def ordered(w):
        return w.reshape(zh, rows, col, -1).transpose(1, 0, 2, 3).reshape(width, -1)

    units = w_gate.shape[2]
    fill = ((0, 0), (0, LANES - units))
    gate_up = jnp.concatenate(
        [jnp.pad(ordered(w_gate[0]), fill), jnp.pad(ordered(w_up[0]), fill)], axis=1
    )
    down = jnp.pad(w_down[0], fill[::-1])
    weights_of = [(gate_up, down), tuple(lax.ppermute(w, "c", [(0, 1), (1, 0)]) for w in (gate_up, down))]

    gain_all = got[:, :, :, used : used + share].transpose(1, 0, 2, 3)
    gain_all = ordered(gain_all.reshape(width, 1)).reshape(rows, 1, LANES)
    rider = part_out.reshape(rows, seq, tp, low * col).transpose(0, 2, 1, 3)
    rider = jnp.pad(rider.astype(bf16), ((0, 0), (0, 0), (0, zh - seq), (0, LANES - low * col)))
    back = experts(block, gain_all, weights_of, rider)
    back = back.reshape(rows * tp, zh, feat + LANES)
    back = exchange(back, PAIR).astype(f32)
    summed = back[:, :, :feat].reshape(chips, c, tp, zh, feat).sum(axis=(0, 2)).astype(bf16)
    returned = exchange(summed.transpose(1, 0, 2), ZH).astype(f32)
    mixer = back[:, :seq, feat : feat + low * col].reshape(rows, tp, seq, low, col).sum(axis=1)
    mixer = mixer.transpose(1, 2, 0, 3).reshape(seq, feat).astype(bf16)
    middle = (tokens.astype(f32) + mixer.astype(f32)).astype(bf16)

    hits = slot_hits(route_experts[None], cap)[:, 0]
    weights = jnp.sum(hits * route_weights[None, :, :, None], axis=2)
    routed = jnp.einsum("ets,esd->td", weights, returned, precision=lax.Precision.HIGHEST)
    mixed = (middle.astype(f32) + routed).astype(bf16)
    return mixed, new_state


def solution(mesh):
    torus = Mesh(mesh.devices.reshape(4, 2, 2, 2, 2, 2, mesh.shape["tp"]), (*EP, "tp"))
    in_specs = (
        P(EP, "tp"),
        P("tp"),
        P("tp", EP),
        P("tp", EP),
        P("tp", EP),
        P("tp"),
        P(),
        P("tp", EP),
        P(EP, "tp", None, None),
        P("tp"),
        P(EP, None),
        P(EP, None),
        P(EP, None, "tp"),
        P(EP, None, "tp"),
        P(EP, "tp", None),
    )
    out_specs = (P(EP, "tp"), P(EP, "tp", None, None))

    return jax.shard_map(
        shards, mesh=torus, in_specs=in_specs, out_specs=out_specs, check_vma=False
    )
```

```python
import jax
import jax.numpy as jnp
from jax import lax
from jax.experimental import pallas as pl
from jax.experimental.pallas import tpu as pltpu
from jax.sharding import Mesh
from jax.sharding import PartitionSpec as P

EXPERTS = 8
EPS = 1e-06
LANES = 128
EP = ("zh", "zl", "xh", "xl", "c")
ROW = ("zl", "xh", "xl", "c")
PAIR = (*ROW, "tp")
GATHER = ("c", "xl", "xh", "zl")
bf16 = jnp.bfloat16
f32 = jnp.float32


def exchange(blocks, axes):
    return lax.all_to_all(blocks, axes, split_axis=0, concat_axis=0, tiled=True)


def gathered(shard, axes, count):
    return exchange(jnp.broadcast_to(shard[None], (count, *shard.shape)), axes)


def slot_hits(experts, cap):
    positions = jnp.arange(experts.shape[1], dtype=jnp.int32)
    earlier = positions[None, :] < positions[:, None]
    same = experts[:, :, :, None, None] == experts[:, None, None, :, :]
    rank = jnp.sum(same & earlier[None, :, None, :, None], axis=(3, 4))
    matched = experts[None] == jnp.arange(EXPERTS, dtype=jnp.int32)[:, None, None, None]
    placed = rank[..., None] == jnp.arange(cap, dtype=jnp.int32)
    return (matched[..., None] & placed[None]).astype(f32)


def chosen_slots(experts, cap):
    return jnp.sum(slot_hits(experts, cap), axis=3)


def resident(value):
    return pltpu.with_memory_space_constraint(value, pltpu.VMEM)


def recurrence_kernel(
    width, got_ref, held, floor_ref, gain_ref, out_ref, forget_ref, input_ref
):
    sources, parts, seq, lanes = got_ref.shape
    heads = forget_ref.shape[0]
    half = sources // 2
    col = lanes // half
    summed = []
    for s in range(half):
        both = []
        for source in (s, s + half):
            block = got_ref[source, 0]
            for part in range(1, parts):
                block = block + got_ref[source, part]
            both.append(block)
        summed.append(jnp.concatenate(both, axis=0))
    stat = summed[0][:seq, lanes - 1 :]
    scale = lax.rsqrt(stat / width + EPS)
    scale = jnp.concatenate([scale, scale], axis=0)
    lane = lax.broadcasted_iota(jnp.int32, (2 * seq, lanes), 1) // col
    first = lax.broadcasted_iota(jnp.int32, (2 * seq, lanes), 0) < seq

    def columns(low, which):
        total = jnp.zeros((2 * seq, lanes), f32)
        at = (low * 3 + which) * col
        for s in range(half):
            moved = pltpu.roll(summed[s], (s * col - at) % lanes, 1)
            total = jnp.where(lane == s, moved, total)
        return total * scale

    rows = []
    for low in range(heads // 2):
        query, gate, value = (columns(low, which) for which in range(3))
        floor = jnp.where(first, floor_ref[2 * low][None, :], floor_ref[2 * low + 1][None, :])
        forget = floor + (1.0 - floor) / (1.0 + jnp.exp(-gate))
        query = query / (1.0 + jnp.exp(-query))
        for k in range(2):
            forget_ref[2 * low + k] = forget[k * seq : (k + 1) * seq]
            input_ref[2 * low + k] = value[k * seq : (k + 1) * seq]
        fresh = jnp.sum(query * (1.0 - forget), axis=1, keepdims=True)
        rows.append((fresh * value, (query * forget).T))
    gain = gain_ref[...].astype(f32)
    for low in range(heads // 2):
        fresh, kept = rows[low]
        old = []
        for k in range(2):
            for t in range(seq):
                r = k * seq + t
                old.append(
                    jnp.sum(kept[:, r : r + 1] * held[t, 2 * low + k], axis=0, keepdims=True)
                )
        reads = fresh + jnp.concatenate(old, axis=0)
        mean_sq = jnp.mean(reads * reads, axis=1, keepdims=True)
        normed = (reads * lax.rsqrt(mean_sq + EPS) * gain).astype(bf16)
        for k in range(2):
            head = 2 * low + k
            block = normed[k * seq : (k + 1) * seq]
            for n in range(out_ref.shape[0]):
                out_ref[n, :, head * lanes : (head + 1) * lanes] = block


def recurrence(width, got, state, floors, gain):
    sources, _, seq, lanes = got.shape
    heads = state.shape[1]
    return pl.pallas_call(
        lambda *refs: recurrence_kernel(width, *refs),
        out_shape=(
            jax.ShapeDtypeStruct((sources, seq, heads * lanes), bf16),
            jax.ShapeDtypeStruct((heads, seq, lanes), f32),
            jax.ShapeDtypeStruct((heads, seq, lanes), f32),
        ),
        in_specs=[
            pl.BlockSpec(memory_space=pltpu.VMEM),
            pl.BlockSpec(memory_space=pltpu.VMEM),
            pl.BlockSpec(memory_space=pltpu.VMEM),
            pl.BlockSpec(memory_space=pltpu.VMEM),
        ],
        out_specs=tuple(pl.BlockSpec(memory_space=pltpu.VMEM) for _ in range(3)),
        name="recurrence",
    )(resident(got), resident(state), floors, gain)


def experts_kernel(
    rows_v, gain_ref, gu0_ref, down0_ref, gu1_ref, down1_ref, rider_ref, out_ref,
    second, gu_v, down_v, out_v, sems, out_sems,
):
    copies = [
        pltpu.make_async_copy(src, dst, sems.at[n])
        for n, (src, dst) in enumerate(
            (
                (gu0_ref, gu_v.at[0]),
                (gu1_ref, gu_v.at[1]),
                (down0_ref, down_v.at[0]),
                (down1_ref, down_v.at[1]),
            )
        )
    ]
    for copy in copies:
        copy.start()
    sources, parts, height, lanes = rows_v.shape
    count = parts * height
    zh, feat = out_v.shape[2], out_v.shape[3] - lanes
    out_v[:, :, :, feat:] = rider_ref[...]
    total = jnp.zeros((count, lanes), f32)
    for n in range(sources):
        block = rows_v[n].reshape(count, lanes).astype(f32)
        total = total + block * block
    scale = lax.rsqrt(jnp.sum(total, axis=1, keepdims=True) / (sources * lanes) + EPS)
    for n in range(sources):
        block = rows_v[n].reshape(count, lanes).astype(f32)
        second[:, n * lanes : (n + 1) * lanes] = (block * scale * gain_ref[n]).astype(bf16)
    hidden = []
    for k in range(2):
        copies[k].wait()
        both = jnp.dot(second[...], gu_v[k], preferred_element_type=f32)
        gate = both[:, :lanes]
        hidden.append((gate / (1.0 + jnp.exp(-gate)) * both[:, lanes:]).astype(bf16))
    copies[2].wait()
    copies[3].wait()
    outs = []
    for part in range(parts):
        at = slice(part * feat, (part + 1) * feat)
        piece = jnp.dot(hidden[0], down_v[0, :, at], preferred_element_type=f32)
        piece = piece + jnp.dot(hidden[1], down_v[1, :, at], preferred_element_type=f32)
        out_v[:, part, :, :feat] = piece.astype(bf16).reshape(count // zh, zh, feat)
        outs.append(pltpu.make_async_copy(out_v.at[:, part], out_ref.at[:, part], out_sems.at[part]))
        outs[-1].start()
    for copy in outs:
        copy.wait()


def experts(block, gain, weights_of, rider):
    sources, parts, height, lanes = block.shape
    (gate_up, down), (gate_up_1, down_1) = weights_of
    zh = rider.shape[2]
    feat = gate_up.shape[0] // parts
    count = parts * height
    whole = (count // zh, parts, zh, feat + lanes)
    anywhere = pl.BlockSpec(memory_space=pl.ANY)
    vmem = pl.BlockSpec(memory_space=pltpu.VMEM)
    return pl.pallas_call(
        experts_kernel,
        out_shape=jax.ShapeDtypeStruct(whole, bf16),
        in_specs=[vmem, vmem, anywhere, anywhere, anywhere, anywhere, vmem],
        out_specs=anywhere,
        scratch_shapes=[
            pltpu.VMEM((count, gate_up.shape[0]), bf16),
            pltpu.VMEM((2, *gate_up.shape), bf16),
            pltpu.VMEM((2, *down.shape), bf16),
            pltpu.VMEM(whole, bf16),
            pltpu.SemaphoreType.DMA((4,)),
            pltpu.SemaphoreType.DMA((parts,)),
        ],
        name="experts",
    )(resident(block), gain, gate_up, down, gate_up_1, down_1, rider)


def shards(
    tokens,
    norm_gain,
    w_query,
    w_forget,
    w_input,
    forget_floor,
    head_gain,
    w_output,
    state,
    ffn_gain,
    route_experts,
    route_weights,
    w_gate,
    w_up,
    w_down,
):
    tp = lax.axis_size("tp")
    rows = lax.axis_size(ROW)
    zh = lax.axis_size("zh")
    seq, feat = tokens.shape
    width = feat * tp
    heads, head = state.shape[1], state.shape[2]
    col = w_query.shape[1]
    low = zh // tp
    here = lax.axis_index(ROW)
    c = lax.axis_size("c")
    chips = rows // c
    cap = max(2, seq // 2)

    w_joint = jnp.concatenate([w_query, w_forget, w_input, w_output], axis=1).T
    w_all = gathered(w_joint, "zh", zh)

    routes = jnp.pad(route_experts.astype(bf16), ((0, 0), (0, feat - route_experts.shape[1])))
    all_rows = jnp.concatenate([tokens, routes], axis=0)
    for axis in GATHER:
        all_rows = lax.all_gather(all_rows, axis, tiled=True)

    def ordered(w):
        return w.reshape(zh, rows, col, -1).transpose(1, 0, 2, 3).reshape(width, -1)

    units = w_gate.shape[2]
    fill = ((0, 0), (0, LANES - units))
    gate_up = jnp.concatenate(
        [jnp.pad(ordered(w_gate[0]), fill), jnp.pad(ordered(w_up[0]), fill)], axis=1
    )
    down = jnp.pad(w_down[0], fill[::-1])
    weights_of = [(gate_up, down), tuple(lax.ppermute(w, "c", [(0, 1), (1, 0)]) for w in (gate_up, down))]

    all_rows = all_rows.reshape(2, 2, 2, 2, 2, seq, feat)
    order = tuple(GATHER[::-1].index(axis) for axis in ROW)
    all_rows = all_rows.transpose(*order, 4, 5, 6).reshape(rows, 2, seq, feat)
    experts_all = all_rows[:, 1, :, : route_experts.shape[1]].astype(jnp.int32)
    w_all, tok_all, weights_of = lax.optimization_barrier(
        (w_all, all_rows[:, 0].reshape(rows * seq, feat), weights_of)
    )
    w_in = w_all[:, : 3 * col].reshape(tp, low * 3 * col, feat)
    w_out = w_all[:, 3 * col :].reshape(tp, low * col, feat)

    tok_all = tok_all.astype(f32)
    sum_sq = jnp.sum(tok_all * tok_all, axis=1)
    scaled = (tok_all * norm_gain.astype(f32)).astype(bf16)
    partial = jnp.einsum("td,pcd->tpc", scaled, w_in, preferred_element_type=f32)
    partial = partial.reshape(rows, seq, tp, low * 3 * col).transpose(0, 2, 1, 3)
    used = low * 3 * col
    share = feat // (rows * seq)
    gain_here = lax.dynamic_index_in_dim(
        ffn_gain.astype(f32).reshape(rows, seq, share), here, 0, False
    )
    gain_sent = jnp.broadcast_to(gain_here, (rows, tp, seq, share))
    stat = jnp.broadcast_to(sum_sq.reshape(rows, 1, seq, 1), (rows, tp, seq, LANES - used - share))
    sent = jnp.concatenate([partial, gain_sent, stat], axis=3).reshape(rows * tp, seq, LANES)
    got = exchange(sent, PAIR).reshape(rows, tp, seq, LANES)

    heads_sent, forget, inputs = recurrence(
        width, got, state, forget_floor.reshape(heads, head), head_gain.reshape(1, head)
    )
    forget, inputs = forget.transpose(1, 0, 2), inputs.transpose(1, 0, 2)
    new_state = forget[..., None] * state + (1.0 - forget)[..., None] * inputs[:, :, None, :]

    quarter = rows // tp
    sel = chosen_slots(experts_all, cap).reshape(EXPERTS, tp, quarter, seq, cap)
    sel = sel.transpose(0, 1, 4, 2, 3)
    eye = jnp.eye(rows, dtype=f32).reshape(tp, quarter, rows)
    sel = sel[:, :, :, :, None, :] * eye[None, :, None, :, :, None]
    sel = sel.reshape(EXPERTS * rows * cap, rows * seq).astype(bf16)

    heads_all = exchange(heads_sent, ROW).reshape(rows * seq, feat)
    part_out = jnp.einsum("td,pcd->tpc", heads_all, w_out, preferred_element_type=f32)
    residual = lax.dynamic_index_in_dim(
        tok_all.reshape(rows * seq, low, rows, col), here, 2, False
    ).reshape(rows * seq, 1, low * col)
    own = (jnp.arange(tp) == lax.axis_index("tp"))[None, :, None]
    with_tok = (part_out + jnp.where(own, residual, 0.0)).reshape(rows * seq, tp * low * col)

    outgoing = jnp.dot(sel, with_tok.astype(bf16), preferred_element_type=f32).astype(bf16)
    arrived = exchange(outgoing.reshape(zh * tp, cap * quarter, LANES), ("zh", "tp"))
    arrived = arrived.astype(f32).reshape(zh, tp, cap, quarter, LANES).sum(axis=1).astype(bf16)
    arrived = arrived.transpose(1, 2, 0, 3).reshape(cap, quarter * zh, LANES)
    sent = jnp.broadcast_to(
        arrived[None, :, None], (chips, c, tp, quarter * zh, LANES)
    ).reshape(rows * tp, quarter * zh, LANES)
    block = exchange(sent, PAIR).reshape(rows, tp, quarter * zh, LANES)

    gain_all = got[:, :, :, used : used + share].transpose(1, 0, 2, 3)
    gain_all = ordered(gain_all.reshape(width, 1)).reshape(rows, 1, LANES)
    rider = part_out.reshape(rows, seq, tp, low * col).transpose(0, 2, 1, 3)
    rider = jnp.pad(rider.astype(bf16), ((0, 0), (0, 0), (0, zh - seq), (0, LANES - low * col)))
    back = experts(block, gain_all, weights_of, rider)
    back = back.reshape(rows * tp, zh, feat + LANES)
    back = exchange(back, PAIR).astype(f32)
    summed = back[:, :, :feat].reshape(chips, c, tp, zh, feat).sum(axis=(0, 2)).astype(bf16)
    returned = exchange(summed.transpose(1, 0, 2), "zh").astype(f32)
    mixer = back[:, :seq, feat : feat + low * col].reshape(rows, tp, seq, low, col).sum(axis=1)
    mixer = mixer.transpose(1, 2, 0, 3).reshape(seq, feat).astype(bf16)
    middle = (tokens.astype(f32) + mixer.astype(f32)).astype(bf16)

    hits = slot_hits(route_experts[None], cap)[:, 0]
    weights = jnp.sum(hits * route_weights[None, :, :, None], axis=2)
    routed = jnp.einsum("ets,esd->td", weights, returned, precision=lax.Precision.HIGHEST)
    mixed = (middle.astype(f32) + routed).astype(bf16)
    return mixed, new_state


def solution(mesh):
    torus = Mesh(mesh.devices.reshape(8, 2, 2, 2, 2, mesh.shape["tp"]), (*EP, "tp"))
    in_specs = (
        P(EP, "tp"),
        P("tp"),
        P("tp", EP),
        P("tp", EP),
        P("tp", EP),
        P("tp"),
        P(),
        P("tp", EP),
        P(EP, "tp", None, None),
        P("tp"),
        P(EP, None),
        P(EP, None),
        P(EP, None, "tp"),
        P(EP, None, "tp"),
        P(EP, "tp", None),
    )
    out_specs = (P(EP, "tp"), P(EP, "tp", None, None))
    return jax.shard_map(
        shards, mesh=torus, in_specs=in_specs, out_specs=out_specs, check_vma=False
    )
```

```python
import jax
import jax.numpy as jnp
from jax import lax
from jax.experimental import pallas as pl
from jax.experimental.pallas import tpu as pltpu
from jax.sharding import Mesh
from jax.sharding import PartitionSpec as P

EXPERTS = 8
EPS = 1e-06
LANES = 128
EP = ("zh", "zl", "xh", "xl", "c")
ROW = ("zl", "xh", "xl", "c")
PAIR = (*ROW, "tp")
GATHER = ("c", "xl", "xh", "zl")
bf16 = jnp.bfloat16
f32 = jnp.float32


def exchange(blocks, axes):
    return lax.all_to_all(blocks, axes, split_axis=0, concat_axis=0, tiled=True)


def gathered(shard, axes, count):
    return exchange(jnp.broadcast_to(shard[None], (count, *shard.shape)), axes)


def slot_hits(experts, cap):
    positions = jnp.arange(experts.shape[1], dtype=jnp.int32)
    earlier = positions[None, :] < positions[:, None]
    same = experts[:, :, :, None, None] == experts[:, None, None, :, :]
    rank = jnp.sum(same & earlier[None, :, None, :, None], axis=(3, 4))
    matched = experts[None] == jnp.arange(EXPERTS, dtype=jnp.int32)[:, None, None, None]
    placed = rank[..., None] == jnp.arange(cap, dtype=jnp.int32)
    return (matched[..., None] & placed[None]).astype(f32)


def chosen_slots(experts, cap):
    return jnp.sum(slot_hits(experts, cap), axis=3)


def resident(value):
    return pltpu.with_memory_space_constraint(value, pltpu.VMEM)


def recurrence_kernel(
    width, got_ref, held, floor_ref, gain_ref, out_ref, forget_ref, input_ref
):
    sources, parts, seq, lanes = got_ref.shape
    heads = forget_ref.shape[0]
    half = sources // 2
    col = lanes // half
    summed = []
    for s in range(half):
        both = []
        for source in (s, s + half):
            block = got_ref[source, 0]
            for part in range(1, parts):
                block = block + got_ref[source, part]
            both.append(block)
        summed.append(jnp.concatenate(both, axis=0))
    stat = summed[0][:seq, lanes - 1 :]
    scale = lax.rsqrt(stat / width + EPS)
    scale = jnp.concatenate([scale, scale], axis=0)
    lane = lax.broadcasted_iota(jnp.int32, (2 * seq, lanes), 1) // col
    first = lax.broadcasted_iota(jnp.int32, (2 * seq, lanes), 0) < seq

    def columns(low, which):
        total = jnp.zeros((2 * seq, lanes), f32)
        at = (low * 3 + which) * col
        for s in range(half):
            moved = pltpu.roll(summed[s], (s * col - at) % lanes, 1)
            total = jnp.where(lane == s, moved, total)
        return total * scale

    rows = []
    for low in range(heads // 2):
        query, gate, value = (columns(low, which) for which in range(3))
        floor = jnp.where(first, floor_ref[2 * low][None, :], floor_ref[2 * low + 1][None, :])
        forget = floor + (1.0 - floor) / (1.0 + jnp.exp(-gate))
        query = query / (1.0 + jnp.exp(-query))
        for k in range(2):
            forget_ref[2 * low + k] = forget[k * seq : (k + 1) * seq]
            input_ref[2 * low + k] = value[k * seq : (k + 1) * seq]
        fresh = jnp.sum(query * (1.0 - forget), axis=1, keepdims=True)
        rows.append((fresh * value, (query * forget).T))
    gain = gain_ref[...].astype(f32)
    for low in range(heads // 2):
        fresh, kept = rows[low]
        old = []
        for k in range(2):
            for t in range(seq):
                r = k * seq + t
                old.append(
                    jnp.sum(kept[:, r : r + 1] * held[t, 2 * low + k], axis=0, keepdims=True)
                )
        reads = fresh + jnp.concatenate(old, axis=0)
        mean_sq = jnp.mean(reads * reads, axis=1, keepdims=True)
        normed = (reads * lax.rsqrt(mean_sq + EPS) * gain).astype(bf16)
        for k in range(2):
            head = 2 * low + k
            block = normed[k * seq : (k + 1) * seq]
            for n in range(out_ref.shape[0]):
                out_ref[n, :, head * lanes : (head + 1) * lanes] = block


def recurrence(width, got, state, floors, gain):
    sources, _, seq, lanes = got.shape
    heads = state.shape[1]
    return pl.pallas_call(
        lambda *refs: recurrence_kernel(width, *refs),
        out_shape=(
            jax.ShapeDtypeStruct((sources, seq, heads * lanes), bf16),
            jax.ShapeDtypeStruct((heads, seq, lanes), f32),
            jax.ShapeDtypeStruct((heads, seq, lanes), f32),
        ),
        in_specs=[
            pl.BlockSpec(memory_space=pltpu.VMEM),
            pl.BlockSpec(memory_space=pltpu.VMEM),
            pl.BlockSpec(memory_space=pltpu.VMEM),
            pl.BlockSpec(memory_space=pltpu.VMEM),
        ],
        out_specs=tuple(pl.BlockSpec(memory_space=pltpu.VMEM) for _ in range(3)),
        compiler_params=pltpu.CompilerParams(vmem_limit_bytes=16 << 20),
        name="recurrence",
    )(resident(got), resident(state), floors, gain)


def experts_kernel(
    rows_v, gain_ref, gu0_ref, down0_ref, gu1_any, down1_any, rider_ref, out_ref,
    second, gu1_ref, down1_ref, out_v, sems, out_sems,
):
    copies = (
        pltpu.make_async_copy(gu1_any, gu1_ref, sems.at[0]),
        pltpu.make_async_copy(down1_any, down1_ref, sems.at[1]),
    )
    for copy in copies:
        copy.start()
    sources, parts, height, lanes = rows_v.shape
    count = parts * height
    zh, feat = out_v.shape[2], out_v.shape[3] - lanes
    out_v[:, :, :, feat:] = rider_ref[...]
    total = jnp.zeros((count, lanes), f32)
    for n in range(sources):
        block = rows_v[n].reshape(count, lanes).astype(f32)
        total = total + block * block
    scale = lax.rsqrt(jnp.sum(total, axis=1, keepdims=True) / (sources * lanes) + EPS)
    for n in range(sources):
        block = rows_v[n].reshape(count, lanes).astype(f32)
        second[:, n * lanes : (n + 1) * lanes] = (block * scale * gain_ref[n]).astype(bf16)
    hidden = []
    for gu_ref in (gu0_ref, gu1_ref):
        if gu_ref is gu1_ref:
            copies[0].wait()
        both = jnp.dot(second[...], gu_ref[...], preferred_element_type=f32)
        gate = both[:, :lanes]
        hidden.append((gate / (1.0 + jnp.exp(-gate)) * both[:, lanes:]).astype(bf16))
    copies[1].wait()
    outs = []
    for part in range(parts):
        at = slice(part * feat, (part + 1) * feat)
        piece = jnp.dot(hidden[0], down0_ref[:, at], preferred_element_type=f32)
        piece = piece + jnp.dot(hidden[1], down1_ref[:, at], preferred_element_type=f32)
        out_v[:, part, :, :feat] = piece.astype(bf16).reshape(count // zh, zh, feat)
        outs.append(pltpu.make_async_copy(out_v.at[:, part], out_ref.at[:, part], out_sems.at[part]))
        outs[-1].start()
    for copy in outs:
        copy.wait()


def experts(block, gain, weights_of, rider):
    sources, parts, height, lanes = block.shape
    (gate_up, down), (gate_up_1, down_1) = weights_of
    zh = rider.shape[2]
    feat = gate_up.shape[0] // parts
    count = parts * height
    whole = (count // zh, parts, zh, feat + lanes)
    anywhere = pl.BlockSpec(memory_space=pl.ANY)
    vmem = pl.BlockSpec(memory_space=pltpu.VMEM)
    return pl.pallas_call(
        experts_kernel,
        out_shape=jax.ShapeDtypeStruct(whole, bf16),
        in_specs=[vmem, vmem, vmem, vmem, anywhere, anywhere, vmem],
        out_specs=anywhere,
        scratch_shapes=[
            pltpu.VMEM((count, gate_up.shape[0]), bf16),
            pltpu.VMEM(gate_up.shape, bf16),
            pltpu.VMEM(down.shape, bf16),
            pltpu.VMEM(whole, bf16),
            pltpu.SemaphoreType.DMA((2,)),
            pltpu.SemaphoreType.DMA((parts,)),
        ],
        compiler_params=pltpu.CompilerParams(vmem_limit_bytes=16 << 20),
        name="experts",
    )(*(resident(v) for v in (block, gain, gate_up, down)), gate_up_1, down_1, resident(rider))


def shards(
    tokens,
    norm_gain,
    w_query,
    w_forget,
    w_input,
    forget_floor,
    head_gain,
    w_output,
    state,
    ffn_gain,
    route_experts,
    route_weights,
    w_gate,
    w_up,
    w_down,
):
    tp = lax.axis_size("tp")
    rows = lax.axis_size(ROW)
    zh = lax.axis_size("zh")
    seq, feat = tokens.shape
    width = feat * tp
    heads, head = state.shape[1], state.shape[2]
    col = w_query.shape[1]
    low = zh // tp
    here = lax.axis_index(ROW)
    c = lax.axis_size("c")
    chips = rows // c
    cap = max(2, seq // 2)

    w_joint = jnp.concatenate([w_query, w_forget, w_input, w_output], axis=1).T
    w_all = gathered(w_joint, "zh", zh)

    routes = jnp.pad(route_experts.astype(bf16), ((0, 0), (0, feat - route_experts.shape[1])))
    all_rows = jnp.concatenate([tokens, routes], axis=0)
    for axis in GATHER:
        all_rows = lax.all_gather(all_rows, axis, tiled=True)

    all_rows = all_rows.reshape(2, 2, 2, 2, 2, seq, feat)
    order = tuple(GATHER[::-1].index(axis) for axis in ROW)
    all_rows = all_rows.transpose(*order, 4, 5, 6).reshape(rows, 2, seq, feat)
    experts_all = all_rows[:, 1, :, : route_experts.shape[1]].astype(jnp.int32)
    w_all, tok_all = lax.optimization_barrier((w_all, all_rows[:, 0].reshape(rows * seq, feat)))
    w_in = w_all[:, : 3 * col].reshape(tp, low * 3 * col, feat)
    w_out = w_all[:, 3 * col :].reshape(tp, low * col, feat)

    tok_all = tok_all.astype(f32)
    sum_sq = jnp.sum(tok_all * tok_all, axis=1)
    scaled = (tok_all * norm_gain.astype(f32)).astype(bf16)
    partial = jnp.einsum("td,pcd->tpc", scaled, w_in, preferred_element_type=f32)
    partial = partial.reshape(rows, seq, tp, low * 3 * col).transpose(0, 2, 1, 3)
    used = low * 3 * col
    share = feat // (rows * seq)
    gain_here = lax.dynamic_index_in_dim(
        ffn_gain.astype(f32).reshape(rows, seq, share), here, 0, False
    )
    gain_sent = jnp.broadcast_to(gain_here, (rows, tp, seq, share))
    stat = jnp.broadcast_to(sum_sq.reshape(rows, 1, seq, 1), (rows, tp, seq, LANES - used - share))
    sent = jnp.concatenate([partial, gain_sent, stat], axis=3).reshape(rows * tp, seq, LANES)
    got = exchange(sent, PAIR).reshape(rows, tp, seq, LANES)

    heads_sent, forget, inputs = recurrence(
        width, got, state, forget_floor.reshape(heads, head), head_gain.reshape(1, head)
    )
    forget, inputs = forget.transpose(1, 0, 2), inputs.transpose(1, 0, 2)
    new_state = forget[..., None] * state + (1.0 - forget)[..., None] * inputs[:, :, None, :]

    quarter = rows // tp
    sel = chosen_slots(experts_all, cap).reshape(EXPERTS, tp, quarter, seq, cap)
    sel = sel.transpose(0, 1, 4, 2, 3)
    eye = jnp.eye(rows, dtype=f32).reshape(tp, quarter, rows)
    sel = sel[:, :, :, :, None, :] * eye[None, :, None, :, :, None]
    sel = sel.reshape(EXPERTS * rows * cap, rows * seq).astype(bf16)

    heads_all = exchange(heads_sent, ROW).reshape(rows * seq, feat)
    part_out = jnp.einsum("td,pcd->tpc", heads_all, w_out, preferred_element_type=f32)
    residual = lax.dynamic_index_in_dim(
        tok_all.reshape(rows * seq, low, rows, col), here, 2, False
    ).reshape(rows * seq, 1, low * col)
    own = (jnp.arange(tp) == lax.axis_index("tp"))[None, :, None]
    with_tok = (part_out + jnp.where(own, residual, 0.0)).reshape(rows * seq, tp * low * col)

    outgoing = jnp.dot(sel, with_tok.astype(bf16), preferred_element_type=f32).astype(bf16)
    arrived = exchange(outgoing.reshape(zh * tp, cap * quarter, LANES), ("zh", "tp"))
    arrived = arrived.astype(f32).reshape(zh, tp, cap, quarter, LANES).sum(axis=1).astype(bf16)
    arrived = arrived.transpose(1, 2, 0, 3).reshape(cap, quarter * zh, LANES)
    sent = jnp.broadcast_to(
        arrived[None, :, None], (chips, c, tp, quarter * zh, LANES)
    ).reshape(rows * tp, quarter * zh, LANES)
    block = exchange(sent, PAIR).reshape(rows, tp, quarter * zh, LANES)

    def ordered(w):
        return w.reshape(zh, rows, col, -1).transpose(1, 0, 2, 3).reshape(width, -1)

    units = w_gate.shape[2]
    fill = ((0, 0), (0, LANES - units))
    gate_up = jnp.concatenate(
        [jnp.pad(ordered(w_gate[0]), fill), jnp.pad(ordered(w_up[0]), fill)], axis=1
    )
    down = jnp.pad(w_down[0], fill[::-1])
    weights_of = [(gate_up, down), tuple(lax.ppermute(w, "c", [(0, 1), (1, 0)]) for w in (gate_up, down))]

    gain_all = got[:, :, :, used : used + share].transpose(1, 0, 2, 3)
    gain_all = ordered(gain_all.reshape(width, 1)).reshape(rows, 1, LANES)
    rider = part_out.reshape(rows, seq, tp, low * col).transpose(0, 2, 1, 3)
    rider = jnp.pad(rider.astype(bf16), ((0, 0), (0, 0), (0, zh - seq), (0, LANES - low * col)))
    back = experts(block, gain_all, weights_of, rider)
    back = back.reshape(rows * tp, zh, feat + LANES)
    back = exchange(back, PAIR).astype(f32)
    summed = back[:, :, :feat].reshape(chips, c, tp, zh, feat).sum(axis=(0, 2)).astype(bf16)
    returned = exchange(summed.transpose(1, 0, 2), "zh").astype(f32)
    mixer = back[:, :seq, feat : feat + low * col].reshape(rows, tp, seq, low, col).sum(axis=1)
    mixer = mixer.transpose(1, 2, 0, 3).reshape(seq, feat).astype(bf16)
    middle = (tokens.astype(f32) + mixer.astype(f32)).astype(bf16)

    hits = slot_hits(route_experts[None], cap)[:, 0]
    weights = jnp.sum(hits * route_weights[None, :, :, None], axis=2)
    routed = jnp.einsum("ets,esd->td", weights, returned, precision=lax.Precision.HIGHEST)
    mixed = (middle.astype(f32) + routed).astype(bf16)
    return mixed, new_state


def solution(mesh):
    torus = Mesh(mesh.devices.reshape(8, 2, 2, 2, 2, mesh.shape["tp"]), (*EP, "tp"))
    in_specs = (
        P(EP, "tp"),
        P("tp"),
        P("tp", EP),
        P("tp", EP),
        P("tp", EP),
        P("tp"),
        P(),
        P("tp", EP),
        P(EP, "tp", None, None),
        P("tp"),
        P(EP, None),
        P(EP, None),
        P(EP, None, "tp"),
        P(EP, None, "tp"),
        P(EP, "tp", None),
    )
    out_specs = (P(EP, "tp"), P(EP, "tp", None, None))
    return jax.shard_map(
        shards, mesh=torus, in_specs=in_specs, out_specs=out_specs, check_vma=False
    )
```

```python
import jax
import jax.numpy as jnp
from jax import lax
from jax.experimental import pallas as pl
from jax.experimental.pallas import tpu as pltpu
from jax.sharding import Mesh
from jax.sharding import PartitionSpec as P

EXPERTS = 8
EPS = 1e-06
LANES = 128
EP = ("zh", "zl", "xh", "xl", "c")
ROW = ("zl", "xh", "xl", "c")
PAIR = (*ROW, "tp")
GATHER = ("c", "xl", "xh", "zl")
bf16 = jnp.bfloat16
f32 = jnp.float32


def exchange(blocks, axes):
    return lax.all_to_all(blocks, axes, split_axis=0, concat_axis=0, tiled=True)


def gathered(shard, axes, count):
    return exchange(jnp.broadcast_to(shard[None], (count, *shard.shape)), axes)


def slot_hits(experts, cap):
    positions = jnp.arange(experts.shape[1], dtype=jnp.int32)
    earlier = positions[None, :] < positions[:, None]
    same = experts[:, :, :, None, None] == experts[:, None, None, :, :]
    rank = jnp.sum(same & earlier[None, :, None, :, None], axis=(3, 4))
    matched = experts[None] == jnp.arange(EXPERTS, dtype=jnp.int32)[:, None, None, None]
    placed = rank[..., None] == jnp.arange(cap, dtype=jnp.int32)
    return (matched[..., None] & placed[None]).astype(f32)


def chosen_slots(experts, cap):
    return jnp.sum(slot_hits(experts, cap), axis=3)


def resident(value):
    return pltpu.with_memory_space_constraint(value, pltpu.VMEM)


def recurrence_kernel(
    width, got_ref, held, floor_ref, gain_ref, out_ref, forget_ref, input_ref
):
    sources, parts, seq, lanes = got_ref.shape
    heads = forget_ref.shape[0]
    half = sources // 2
    col = lanes // half
    summed = []
    for s in range(half):
        both = []
        for source in (s, s + half):
            block = got_ref[source, 0]
            for part in range(1, parts):
                block = block + got_ref[source, part]
            both.append(block)
        summed.append(jnp.concatenate(both, axis=0))
    stat = summed[0][:seq, lanes - 1 :]
    scale = lax.rsqrt(stat / width + EPS)
    scale = jnp.concatenate([scale, scale], axis=0)
    lane = lax.broadcasted_iota(jnp.int32, (2 * seq, lanes), 1) // col
    first = lax.broadcasted_iota(jnp.int32, (2 * seq, lanes), 0) < seq

    def columns(low, which):
        total = jnp.zeros((2 * seq, lanes), f32)
        at = (low * 3 + which) * col
        for s in range(half):
            moved = pltpu.roll(summed[s], (s * col - at) % lanes, 1)
            total = jnp.where(lane == s, moved, total)
        return total * scale

    rows = []
    for low in range(heads // 2):
        query, gate, value = (columns(low, which) for which in range(3))
        floor = jnp.where(first, floor_ref[2 * low][None, :], floor_ref[2 * low + 1][None, :])
        forget = floor + (1.0 - floor) / (1.0 + jnp.exp(-gate))
        query = query / (1.0 + jnp.exp(-query))
        for k in range(2):
            forget_ref[2 * low + k] = forget[k * seq : (k + 1) * seq]
            input_ref[2 * low + k] = value[k * seq : (k + 1) * seq]
        fresh = jnp.sum(query * (1.0 - forget), axis=1, keepdims=True)
        rows.append((fresh * value, (query * forget).T))
    gain = gain_ref[...].astype(f32)
    for low in range(heads // 2):
        fresh, kept = rows[low]
        old = []
        for k in range(2):
            for t in range(seq):
                r = k * seq + t
                old.append(
                    jnp.sum(kept[:, r : r + 1] * held[t, 2 * low + k], axis=0, keepdims=True)
                )
        reads = fresh + jnp.concatenate(old, axis=0)
        mean_sq = jnp.mean(reads * reads, axis=1, keepdims=True)
        normed = (reads * lax.rsqrt(mean_sq + EPS) * gain).astype(bf16)
        for k in range(2):
            head = 2 * low + k
            block = normed[k * seq : (k + 1) * seq]
            for n in range(out_ref.shape[0]):
                out_ref[n, :, head * lanes : (head + 1) * lanes] = block


def recurrence(width, got, state, floors, gain):
    sources, _, seq, lanes = got.shape
    heads = state.shape[1]
    return pl.pallas_call(
        lambda *refs: recurrence_kernel(width, *refs),
        out_shape=(
            jax.ShapeDtypeStruct((sources, seq, heads * lanes), bf16),
            jax.ShapeDtypeStruct((heads, seq, lanes), f32),
            jax.ShapeDtypeStruct((heads, seq, lanes), f32),
        ),
        in_specs=[
            pl.BlockSpec(memory_space=pltpu.VMEM),
            pl.BlockSpec(memory_space=pltpu.VMEM),
            pl.BlockSpec(memory_space=pltpu.VMEM),
            pl.BlockSpec(memory_space=pltpu.VMEM),
        ],
        out_specs=tuple(pl.BlockSpec(memory_space=pltpu.VMEM) for _ in range(3)),
        compiler_params=pltpu.CompilerParams(vmem_limit_bytes=16 << 20),
        name="recurrence",
    )(resident(got), resident(state), floors, gain)


def experts_kernel(
    rows_v, gain_ref, gu0_ref, down0_any, gu1_any, down1_any, rider_ref, out_ref,
    second, gu1_ref, down0_ref, down1_ref, out_v, sems, out_sems,
):
    copies = (
        pltpu.make_async_copy(gu1_any, gu1_ref, sems.at[0]),
        pltpu.make_async_copy(down0_any, down0_ref, sems.at[1]),
        pltpu.make_async_copy(down1_any, down1_ref, sems.at[2]),
    )
    for copy in copies:
        copy.start()
    sources, parts, height, lanes = rows_v.shape
    count = parts * height
    zh, feat = out_v.shape[2], out_v.shape[3] - lanes
    out_v[:, :, :, feat:] = rider_ref[...]
    total = jnp.zeros((count, lanes), f32)
    for n in range(sources):
        block = rows_v[n].reshape(count, lanes).astype(f32)
        total = total + block * block
    scale = lax.rsqrt(jnp.sum(total, axis=1, keepdims=True) / (sources * lanes) + EPS)
    for n in range(sources):
        block = rows_v[n].reshape(count, lanes).astype(f32)
        second[:, n * lanes : (n + 1) * lanes] = (block * scale * gain_ref[n]).astype(bf16)
    hidden = []
    for gu_ref in (gu0_ref, gu1_ref):
        if gu_ref is gu1_ref:
            copies[0].wait()
        both = jnp.dot(second[...], gu_ref[...], preferred_element_type=f32)
        gate = both[:, :lanes]
        hidden.append((gate / (1.0 + jnp.exp(-gate)) * both[:, lanes:]).astype(bf16))
    copies[1].wait()
    copies[2].wait()
    outs = []
    for part in range(parts):
        at = slice(part * feat, (part + 1) * feat)
        piece = jnp.dot(hidden[0], down0_ref[:, at], preferred_element_type=f32)
        piece = piece + jnp.dot(hidden[1], down1_ref[:, at], preferred_element_type=f32)
        out_v[:, part, :, :feat] = piece.astype(bf16).reshape(count // zh, zh, feat)
        outs.append(pltpu.make_async_copy(out_v.at[:, part], out_ref.at[:, part], out_sems.at[part]))
        outs[-1].start()
    for copy in outs:
        copy.wait()


def experts(block, gain, weights_of, rider):
    sources, parts, height, lanes = block.shape
    (gate_up, down), (gate_up_1, down_1) = weights_of
    zh = rider.shape[2]
    feat = gate_up.shape[0] // parts
    count = parts * height
    whole = (count // zh, parts, zh, feat + lanes)
    anywhere = pl.BlockSpec(memory_space=pl.ANY)
    far = pl.BlockSpec(memory_space=pltpu.HBM)
    vmem = pl.BlockSpec(memory_space=pltpu.VMEM)
    return pl.pallas_call(
        experts_kernel,
        out_shape=jax.ShapeDtypeStruct(whole, bf16),
        in_specs=[vmem, vmem, vmem, far, far, far, vmem],
        out_specs=anywhere,
        scratch_shapes=[
            pltpu.VMEM((count, gate_up.shape[0]), bf16),
            pltpu.VMEM(gate_up.shape, bf16),
            pltpu.VMEM(down.shape, bf16),
            pltpu.VMEM(down.shape, bf16),
            pltpu.VMEM(whole, bf16),
            pltpu.SemaphoreType.DMA((3,)),
            pltpu.SemaphoreType.DMA((parts,)),
        ],
        compiler_params=pltpu.CompilerParams(vmem_limit_bytes=16 << 20),
        name="experts",
    )(
        *(resident(v) for v in (block, gain, gate_up)),
        *(pltpu.with_memory_space_constraint(v, pltpu.HBM) for v in (down, gate_up_1, down_1)),
        resident(rider),
    )


def shards(
    tokens,
    norm_gain,
    w_query,
    w_forget,
    w_input,
    forget_floor,
    head_gain,
    w_output,
    state,
    ffn_gain,
    route_experts,
    route_weights,
    w_gate,
    w_up,
    w_down,
):
    tp = lax.axis_size("tp")
    rows = lax.axis_size(ROW)
    zh = lax.axis_size("zh")
    seq, feat = tokens.shape
    width = feat * tp
    heads, head = state.shape[1], state.shape[2]
    col = w_query.shape[1]
    low = zh // tp
    here = lax.axis_index(ROW)
    c = lax.axis_size("c")
    chips = rows // c
    cap = max(2, seq // 2)

    w_joint = jnp.concatenate([w_query, w_forget, w_input, w_output], axis=1).T
    w_all = gathered(w_joint, "zh", zh)

    routes = jnp.pad(route_experts.astype(bf16), ((0, 0), (0, feat - route_experts.shape[1])))
    all_rows = jnp.concatenate([tokens, routes], axis=0)
    for axis in GATHER:
        all_rows = lax.all_gather(all_rows, axis, tiled=True)

    swap = [(0, 1), (1, 0)]
    down = jnp.pad(w_down[0], ((0, LANES - w_down.shape[1]), (0, 0)))
    down_other = lax.ppermute(down, "c", swap)
    all_rows = all_rows.reshape(2, 2, 2, 2, 2, seq, feat)
    order = tuple(GATHER[::-1].index(axis) for axis in ROW)
    all_rows = all_rows.transpose(*order, 4, 5, 6).reshape(rows, 2, seq, feat)
    experts_all = all_rows[:, 1, :, : route_experts.shape[1]].astype(jnp.int32)
    w_all, tok_all, down, down_other = lax.optimization_barrier(
        (w_all, all_rows[:, 0].reshape(rows * seq, feat), down, down_other)
    )
    w_in = w_all[:, : 3 * col].reshape(tp, low * 3 * col, feat)
    w_out = w_all[:, 3 * col :].reshape(tp, low * col, feat)

    tok_all = tok_all.astype(f32)
    sum_sq = jnp.sum(tok_all * tok_all, axis=1)
    scaled = (tok_all * norm_gain.astype(f32)).astype(bf16)
    partial = jnp.einsum("td,pcd->tpc", scaled, w_in, preferred_element_type=f32)
    partial = partial.reshape(rows, seq, tp, low * 3 * col).transpose(0, 2, 1, 3)
    used = low * 3 * col
    share = feat // (rows * seq)
    gain_here = lax.dynamic_index_in_dim(
        ffn_gain.astype(f32).reshape(rows, seq, share), here, 0, False
    )
    gain_sent = jnp.broadcast_to(gain_here, (rows, tp, seq, share))
    stat = jnp.broadcast_to(sum_sq.reshape(rows, 1, seq, 1), (rows, tp, seq, LANES - used - share))
    sent = jnp.concatenate([partial, gain_sent, stat], axis=3).reshape(rows * tp, seq, LANES)
    got = exchange(sent, PAIR).reshape(rows, tp, seq, LANES)

    heads_sent, forget, inputs = recurrence(
        width, got, state, forget_floor.reshape(heads, head), head_gain.reshape(1, head)
    )
    forget, inputs = forget.transpose(1, 0, 2), inputs.transpose(1, 0, 2)
    new_state = forget[..., None] * state + (1.0 - forget)[..., None] * inputs[:, :, None, :]

    quarter = rows // tp
    sel = chosen_slots(experts_all, cap).reshape(EXPERTS, tp, quarter, seq, cap)
    sel = sel.transpose(0, 1, 4, 2, 3)
    eye = jnp.eye(rows, dtype=f32).reshape(tp, quarter, rows)
    sel = sel[:, :, :, :, None, :] * eye[None, :, None, :, :, None]
    sel = sel.reshape(EXPERTS * rows * cap, rows * seq).astype(bf16)

    heads_all = exchange(heads_sent, ROW).reshape(rows * seq, feat)
    part_out = jnp.einsum("td,pcd->tpc", heads_all, w_out, preferred_element_type=f32)
    residual = lax.dynamic_index_in_dim(
        tok_all.reshape(rows * seq, low, rows, col), here, 2, False
    ).reshape(rows * seq, 1, low * col)
    own = (jnp.arange(tp) == lax.axis_index("tp"))[None, :, None]
    with_tok = (part_out + jnp.where(own, residual, 0.0)).reshape(rows * seq, tp * low * col)

    outgoing = jnp.dot(sel, with_tok.astype(bf16), preferred_element_type=f32).astype(bf16)
    arrived = exchange(outgoing.reshape(zh * tp, cap * quarter, LANES), ("zh", "tp"))
    arrived = arrived.astype(f32).reshape(zh, tp, cap, quarter, LANES).sum(axis=1).astype(bf16)
    arrived = arrived.transpose(1, 2, 0, 3).reshape(cap, quarter * zh, LANES)
    sent = jnp.broadcast_to(
        arrived[None, :, None], (chips, c, tp, quarter * zh, LANES)
    ).reshape(rows * tp, quarter * zh, LANES)
    block = exchange(sent, PAIR).reshape(rows, tp, quarter * zh, LANES)

    def ordered(w):
        return w.reshape(zh, rows, col, -1).transpose(1, 0, 2, 3).reshape(width, -1)

    units = w_gate.shape[2]
    fill = ((0, 0), (0, LANES - units))
    gate_up = jnp.concatenate(
        [jnp.pad(ordered(w_gate[0]), fill), jnp.pad(ordered(w_up[0]), fill)], axis=1
    )
    weights_of = [(gate_up, down), (lax.ppermute(gate_up, "c", swap), down_other)]

    gain_all = got[:, :, :, used : used + share].transpose(1, 0, 2, 3)
    gain_all = ordered(gain_all.reshape(width, 1)).reshape(rows, 1, LANES)
    rider = part_out.reshape(rows, seq, tp, low * col).transpose(0, 2, 1, 3)
    rider = jnp.pad(rider.astype(bf16), ((0, 0), (0, 0), (0, zh - seq), (0, LANES - low * col)))
    back = experts(block, gain_all, weights_of, rider)
    back = back.reshape(rows * tp, zh, feat + LANES)
    back = exchange(back, PAIR).astype(f32)
    summed = back[:, :, :feat].reshape(chips, c, tp, zh, feat).sum(axis=(0, 2)).astype(bf16)
    returned = exchange(summed.transpose(1, 0, 2), "zh").astype(f32)
    mixer = back[:, :seq, feat : feat + low * col].reshape(rows, tp, seq, low, col).sum(axis=1)
    mixer = mixer.transpose(1, 2, 0, 3).reshape(seq, feat).astype(bf16)
    middle = (tokens.astype(f32) + mixer.astype(f32)).astype(bf16)

    hits = slot_hits(route_experts[None], cap)[:, 0]
    weights = jnp.sum(hits * route_weights[None, :, :, None], axis=2)
    routed = jnp.einsum("ets,esd->td", weights, returned, precision=lax.Precision.HIGHEST)
    mixed = (middle.astype(f32) + routed).astype(bf16)
    return mixed, new_state


def solution(mesh):
    torus = Mesh(mesh.devices.reshape(8, 2, 2, 2, 2, mesh.shape["tp"]), (*EP, "tp"))
    in_specs = (
        P(EP, "tp"),
        P("tp"),
        P("tp", EP),
        P("tp", EP),
        P("tp", EP),
        P("tp"),
        P(),
        P("tp", EP),
        P(EP, "tp", None, None),
        P("tp"),
        P(EP, None),
        P(EP, None),
        P(EP, None, "tp"),
        P(EP, None, "tp"),
        P(EP, "tp", None),
    )
    out_specs = (P(EP, "tp"), P(EP, "tp", None, None))
    return jax.shard_map(
        shards, mesh=torus, in_specs=in_specs, out_specs=out_specs, check_vma=False
    )
```
